32 devices in a mesh: sp: 8 (over z, x), tp: 4 (over y, core).
Axes of the slice: x: 2, y: 2, z: 4, core: 2. Of those that a mesh axis runs over, the one named last changes fastest.
Arguments:
- mixer_out: bfloat16 [1024, 2048], P('sp'), may hold values from -6 to 6
- out_grad: bfloat16 [1024, 2048], P('sp'), may hold values from -2 to 2
- route_ids: int32 [1024, 2], P('sp'), may hold values from 0 to 7, all different within a row; in each aligned block of 128 rows (0 to 127, 128 to 255, ...) at most 64 rows name the same one
- route_weights: float32 [1024, 2], P('sp'), may hold values from 0.2 to 1.2
- gate_branch: bfloat16 [1024, 2048], P('sp', 'tp'), may hold values from -4 to 4
- states: float32 [1024, 2048], P('sp', 'tp'), may hold values from -6 to 6
- decay: float32 [1024, 2048], P('sp', 'tp'), may hold values from 0 to 1
- w_proj: bfloat16 [2048, 2048], P(None, 'tp'), may hold values from -0.125 to 0.125
- w_gate: bfloat16 [8, 2048, 2048], P('sp', 'tp'), may hold values from -0.125 to 0.125
- w_up: bfloat16 [8, 2048, 2048], P('sp', 'tp'), may hold values from -0.125 to 0.125
- w_down: bfloat16 [8, 2048, 2048], P('sp', 'tp'), may hold values from -0.125 to 0.125
Outputs:
- grad_w_gate: bfloat16 [8, 2048, 2048], P('sp', 'tp')
- grad_w_up: bfloat16 [8, 2048, 2048], P('sp', 'tp')
- grad_w_down: bfloat16 [8, 2048, 2048], P('sp', 'tp')
- grad_w_proj: float32 [2048, 2048], P('sp', 'tp')
- grad_branch: bfloat16 [1024, 2048], P('sp', 'tp')
- grad_drive: float32 [1024, 2048], P('sp', 'tp')
- grad_decay: float32 [1024, 2048], P('sp', 'tp')
The draws below stay inside these ranges and needn't reach their ends.
Inputs may be any that keep to these rules, and one draw needn't show every extreme that they name: `route_ids`: each row names 2 different experts. In the rows of one index of sp no expert is named more than 64 times, a bound that some block reaches.
All inputs are finite; a program needn't handle non-finite values.
Results may differ from the reference program's by a relative error of at most 0.02.
Values may be sent and summed in bfloat16 or wider, within the bound.
A program may use at most 64 MiB of HBM per device.

```python
import math
import jax
import jax.numpy as jnp
import numpy as np
from jax import lax

D = 2048
D_RNN = 2048
F = 2048
TOP = 2
TOK_DEV = 128
EXPERTS = 8
TOKENS = 1024
CAP = 64
N_SP = 8
N_TP = 4


def draw_decay(key, part):
    keys = jax.random.split(jax.random.fold_in(key, 17), 5)
    fast_share = 0.5
    fast = jax.random.uniform(keys[0], (D_RNN,), jnp.float32) < fast_share
    slow_rate = jax.random.uniform(keys[1], (D_RNN,), jnp.float32, 0.25, 0.8) / TOKENS
    fast_rate = jnp.exp(jax.random.uniform(keys[2], (D_RNN,), jnp.float32, jnp.log(0.01), jnp.log(1.0 / 30.0)))
    base_rate = jnp.where(fast, fast_rate, slow_rate)
    spans = TOKENS // 64
    factor = jnp.exp(jax.random.uniform(keys[3], (spans, 1), jnp.float32, jnp.log(0.4), jnp.log(1.6)))
    noise = jax.random.uniform(keys[4], (TOKENS, D_RNN), jnp.float32, 0.5, 1.5)
    return jnp.exp(-(base_rate[None, :] * jnp.repeat(factor, 64, axis=0) * noise))


def strengthened(array, own_key, source, target, shards_of, factor):
    owner, partner = [(jnp.arange(array.shape[dim]) // (array.shape[dim] // shards_of)).reshape([-1 if axis == dim else 1 for axis in range(array.ndim)]) for dim in (source, target)]
    chosen = jax.random.permutation(own_key, shards_of)[partner]
    strong = (owner == chosen) | (owner == (partner + shards_of // 2) % shards_of)
    return jnp.where(strong, factor * array, array)


def levels(stream_key, extent, cuts, smallest, largest):
    def one(axis_at, shards_of):
        steps = jax.random.uniform(jax.random.fold_in(jax.random.fold_in(stream_key, 6), axis_at), (shards_of,), jnp.float32, smallest / len(cuts), largest / len(cuts))
        return jnp.repeat(jnp.exp(steps), extent[axis_at] // shards_of).reshape((-1,) + (1,) * (len(extent) - axis_at - 1))

    loudness = one(*cuts[0])
    for cut in cuts[1:]:
        loudness = loudness * one(*cut)
    return loudness


def shared_out(key, own, number, rows, amount, top, most, skew):
    sequence = jax.random.permutation(key, amount)
    crowded, common = shares(amount, rows * top, most, skew, True), shares(amount, rows * top, most, skew, False)
    places = jnp.arange(amount)

    def named(lengths, turn):
        used = int((lengths > 0).sum())
        fixed = max(1, used // 4)
        passed = fixed + (places - fixed + turn * (used - fixed)) % max(1, amount - fixed)
        return jnp.zeros((amount,), jnp.int32).at[sequence[jnp.where(places < fixed, places, passed)]].set(jnp.asarray(lengths, jnp.int32))

    lengths = jnp.where(number % 4 == 0, named(crowded, number // 4), named(common, number - number // 4 - 1))
    mixed = jax.random.permutation(jax.random.fold_in(own, 3), amount)
    giver, receiver = mixed[0:amount // 2 * 2:2], mixed[1:amount // 2 * 2:2]
    margin = jnp.minimum(lengths[giver] - 1, most - lengths[receiver]) // 2
    margin = jnp.where((giver == sequence[0]) | (receiver == sequence[0]) | (lengths[receiver] == 0), 0, jnp.maximum(margin, 0))
    passed = jax.random.randint(jax.random.fold_in(own, 4), (amount // 2,), 0, 1 << 20) % (margin + 1)
    lengths = lengths.at[giver].add(-passed).at[receiver].add(passed)
    items = jnp.searchsorted(jnp.cumsum(lengths), jnp.arange(rows * top), side="right").astype(jnp.int32)
    listing = items.reshape(top, rows).T
    listing = listing[jax.random.permutation(jax.random.fold_in(own, 1), rows)]
    turn = jax.random.randint(jax.random.fold_in(own, 2), (rows, 1), 0, top)
    return jnp.take_along_axis(listing, (jnp.arange(top)[None, :] + turn) % top, axis=1)


def shares(count, total, limit, lean, full):
    weights = [(1 << 20) // math.isqrt(grade ** lean) + 1 for grade in range(1, count + 1)]
    largest = limit if full else min(limit, max(-(-total // count), total * weights[0] // sum(weights)))
    least = 1 if total - largest >= count - 1 else 0
    counts, rest = [largest] + [least] * (count - 1), total - largest - least * (count - 1)
    while rest > 0:
        movable = [i for i in range(1, count) if counts[i] < largest] or [i for i in range(1, count) if counts[i] < limit]
        mass, left = sum([weights[i] for i in movable]), rest
        for i in movable:
            extra = min(limit - counts[i], max(1, left * weights[i] // mass), rest)
            counts[i] = counts[i] + extra
            rest = rest - extra
    return np.array(counts)


def bell_draw(stream_key, dims, width, most, cuts=(), kind=jnp.bfloat16):
    entries = jax.random.normal(stream_key, dims, jnp.float32) * width
    if len(cuts) > 0:
        entries = levels(stream_key, dims, cuts, -0.22, 0.18) * entries
    return jnp.clip(entries, min=-most, max=most).astype(kind)


def noise_with(stream_key, shape, deviation, bound, shards, heavy, kind=jnp.bfloat16):
    entries = deviation * jax.random.normal(stream_key, shape, jnp.float32)
    if shards:
        entries = entries * levels(stream_key, shape, shards, -0.22, 0.18)
    return jnp.clip(strengthened(entries, jax.random.fold_in(stream_key, 3), *heavy), -bound, bound).astype(kind)


def setup_inputs(seed: int = 0) -> dict:
    key_list = jax.random.split(jax.random.key(seed), 12)
    mixer_out = bell_draw(key_list[0], (TOKENS, D), 1.0, 6.0, ((0, 8),))
    out_grad = noise_with(key_list[1], (TOKENS, D), 0.25, 2.0, ((0, 8),), (0, 1, 8, 2.0))
    route_ids_keys = jax.random.split(jax.random.fold_in(key_list[2], 1), TOKENS // TOK_DEV)
    route_ids_turns = jax.random.permutation(jax.random.fold_in(key_list[2], 3), TOKENS // TOK_DEV)
    route_ids = jax.vmap(lambda own, number: shared_out(jax.random.fold_in(key_list[2], 2), own, number, TOK_DEV, EXPERTS, TOP, CAP, 1))(route_ids_keys, route_ids_turns).reshape((TOKENS, TOP))
    route_weights = jnp.clip(0.2 + 1 * jax.random.uniform(key_list[3], (TOKENS, TOP), jnp.float32) ** levels(key_list[3], (TOKENS, TOP), ((0, 8),), -0.2, 0.2), 0.2, 1.2)
    gate_branch = bell_draw(key_list[4], (TOKENS, D_RNN), 0.5, 4.0, ((0, 8), (1, 4)))
    states = bell_draw(key_list[5], (TOKENS, D_RNN), 1.0, 6.0, ((0, 8), (1, 4)), jnp.float32)
    decay = draw_decay(jax.random.fold_in(key_list[11], 71), 0)
    w_proj = bell_draw(key_list[7], (D, D_RNN), D_RNN ** -0.5, 0.125, ((1, 4),))
    w_gate = bell_draw(key_list[8], (EXPERTS, F, D), D ** -0.5, 0.125, ((0, 8), (1, 4)))
    w_up = bell_draw(key_list[9], (EXPERTS, F, D), D ** -0.5, 0.125, ((0, 8), (1, 4)))
    w_down = bell_draw(key_list[10], (EXPERTS, F, D), F ** -0.5, 0.125, ((0, 8), (1, 4)))
    return dict(mixer_out=mixer_out, out_grad=out_grad, route_ids=route_ids, route_weights=route_weights, gate_branch=gate_branch, states=states, decay=decay, w_proj=w_proj, w_gate=w_gate, w_up=w_up, w_down=w_down)


def linear_combine(earlier, later):
    return earlier[0] * later[0], later[0] * earlier[1] + later[1]


def reference(mixer_out, out_grad, route_ids, route_weights, gate_branch, states, decay, w_proj, w_gate, w_up, w_down):
    routes = TOKENS * TOP
    flat_ids = route_ids.reshape(-1).astype(jnp.int32)
    onehot = (flat_ids[:, None] == jnp.arange(EXPERTS, dtype=jnp.int32)[None, :]).astype(jnp.int32)
    counted = jnp.cumsum(onehot.reshape(N_SP, TOK_DEV * TOP, EXPERTS), axis=1).reshape(routes, EXPERTS)
    position = (jnp.sum(counted * onehot, axis=1) - 1).astype(jnp.int32)
    block_id = (jnp.arange(routes, dtype=jnp.int32) // (TOK_DEV * TOP)).astype(jnp.int32)
    slot_index = ((flat_ids * N_SP + block_id) * CAP + position).astype(jnp.int32)
    table = jnp.full((EXPERTS * N_SP * CAP,), routes, jnp.int32).at[slot_index].set(jnp.arange(routes, dtype=jnp.int32))
    table = table.reshape(EXPERTS, N_SP * CAP)
    scaled = (route_weights[:, :, None].astype(jnp.float32) * out_grad[:, None, :].astype(jnp.float32)).astype(jnp.bfloat16)
    scaled_pad = jnp.concatenate([scaled.reshape(routes, D), jnp.zeros((1, D), jnp.bfloat16)], axis=0)
    token_pad = jnp.concatenate([mixer_out, jnp.zeros((1, D), jnp.bfloat16)], axis=0)

    def one_expert(carry, expert):
        slot_routes = table[expert]
        inputs = token_pad[slot_routes // TOP].astype(jnp.float32)
        cotangents = scaled_pad[slot_routes].astype(jnp.float32)
        weight_gate = w_gate[expert].astype(jnp.float32)
        weight_up = w_up[expert].astype(jnp.float32)
        weight_down = w_down[expert].astype(jnp.float32)
        gate_pre = jnp.dot(inputs, weight_gate.T, preferred_element_type=jnp.float32)
        up_pre = jnp.dot(inputs, weight_up.T, preferred_element_type=jnp.float32)
        sigmoid_gate = jax.nn.sigmoid(gate_pre)
        silu_gate = gate_pre * sigmoid_gate
        hidden = (silu_gate * up_pre).astype(jnp.bfloat16).astype(jnp.float32)
        hidden_grad = jnp.dot(cotangents, weight_down.T, preferred_element_type=jnp.float32)
        up_grad = (hidden_grad * silu_gate).astype(jnp.bfloat16).astype(jnp.float32)
        gate_grad = (hidden_grad * up_pre * sigmoid_gate * (1.0 + gate_pre * (1.0 - sigmoid_gate))).astype(jnp.bfloat16).astype(jnp.float32)
        grad_gate = jnp.dot(gate_grad.T, inputs, preferred_element_type=jnp.float32).astype(jnp.bfloat16)
        grad_up = jnp.dot(up_grad.T, inputs, preferred_element_type=jnp.float32).astype(jnp.bfloat16)
        grad_down = jnp.dot(hidden.T, cotangents, preferred_element_type=jnp.float32).astype(jnp.bfloat16)
        slots = slot_routes.shape[0]
        block_part = jnp.einsum("sbf,bfd->sbd", gate_grad.reshape(slots, N_TP, F // N_TP), weight_gate.reshape(N_TP, F // N_TP, D))
        block_part = block_part + jnp.einsum("sbf,bfd->sbd", up_grad.reshape(slots, N_TP, F // N_TP), weight_up.reshape(N_TP, F // N_TP, D))
        partial_value = jnp.sum(block_part.astype(jnp.bfloat16).astype(jnp.float32), axis=1)
        carry = carry.at[slot_routes].add(partial_value)
        return carry, (grad_gate, grad_up, grad_down)

    start_carry = jnp.zeros((routes + 1, D), jnp.float32)
    route_grad, stacked = lax.scan(one_expert, start_carry, jnp.arange(EXPERTS, dtype=jnp.int32))
    grad_w_gate, grad_w_up, grad_w_down = stacked
    routed_grad = jnp.sum(route_grad[:routes].reshape(TOKENS, TOP, D), axis=1)
    mid_grad = (out_grad.astype(jnp.float32) + routed_grad).astype(jnp.bfloat16)
    gated = (gate_branch.astype(jnp.float32) * states).astype(jnp.bfloat16)
    grad_w_proj = jnp.dot(mid_grad.T, gated, preferred_element_type=jnp.float32)
    act_grad = jnp.dot(mid_grad, w_proj, preferred_element_type=jnp.float32)
    grad_branch = (act_grad * states).astype(jnp.bfloat16)
    state_grad = act_grad * gate_branch.astype(jnp.float32)
    next_decay = jnp.concatenate([decay[1:], jnp.ones((1, D_RNN), jnp.float32)], axis=0)
    decay_prod, flipped = lax.associative_scan(linear_combine, (next_decay[::-1], state_grad[::-1]), axis=0)
    grad_drive = flipped[::-1]
    previous = jnp.concatenate([jnp.zeros((1, D_RNN), jnp.float32), states[:-1]], axis=0)
    grad_decay = grad_drive * previous
    return grad_w_gate, grad_w_up, grad_w_down, grad_w_proj, grad_branch, grad_drive, grad_decay
```

```python
import functools

import jax
import jax.numpy as jnp
from jax import lax
from jax.experimental import pallas as pl
from jax.experimental.pallas import tpu as pltpu
from jax.sharding import PartitionSpec as P

MESH = pl.DeviceIdType.MESH
F32 = jnp.float32
BF16 = jnp.bfloat16
LIMIT = 44 * 1024 * 1024


def dot(a, b, ca, cb):
    return lax.dot_general(a, b, (((ca,), (cb,)), ((), ())), preferred_element_type=F32)


def kernel(
    n_sp,
    n_tp,
    ids_h,
    wts_h,
    mix_h,
    og_h,
    gb_h,
    st_h,
    dc_h,
    wp_h,
    wg_h,
    wu_h,
    wd_h,
    dwg,
    dwu,
    dwd,
    gproj,
    gbr,
    gdr,
    gdc,
    ids,
    wts,
    mix,
    og,
    gb,
    st,
    dc,
    wp,
    wg,
    wu,
    wd,
    sel,
    sw,
    send,
    xc,
    ga,
    pv,
    gg,
    ug,
    hid,
    pb,
    po,
    rc,
    qb,
    ry,
    fb,
    ret,
    mt,
    mr,
    cs,
    cr,
    w_sem,
    sp_s,
    sp_r,
    core_s,
    core_r,
    y_s,
    y_r,
    ga_s,
    ga_r,
    pv_sem,
    pc_s,
    pc_r,
    py_s,
    py_r,
    ret_s,
    ret_r,
    mtc_s,
    mtc_r,
    mty_s,
    mty_r,
    mr_s,
    mr_r,
    mrc_s,
    mrc_r,
    c_s,
    c_r,
):
    i = lax.axis_index("sp")
    t = lax.axis_index("tp")
    ny = n_tp // 2
    y, c = t // 2, t % 2
    tok = mix.shape[0]
    cap = xc.shape[3]
    dg = xc.shape[4]
    slots = n_sp * cap
    peer = (i, y * 2 + 1 - c)
    straight = (1,)
    bounds = ((0, n_sp // 2), (n_sp // 2, 3 * n_sp // 4), (3 * n_sp // 4, n_sp))
    scope = jax.named_scope

    def columns(g):
        return pl.ds(pl.multiple_of(g * dg, dg), dg)

    def mate(k):
        to, bit = i, 1
        while bit <= k:
            if k & bit:
                to = to + bit * (1 - 2 * ((i // bit) % 2))
            bit *= 2
        return to

    def y_up(q):
        return lax.rem(y + q, ny)

    def remote(src, dst, s, r, who):
        return pltpu.make_async_remote_copy(
            src_ref=src, dst_ref=dst, send_sem=s, recv_sem=r, device_id=who, device_id_type=MESH
        )

    barrier = pltpu.get_barrier_semaphore()
    for k in range(1, n_sp):
        pl.semaphore_signal(barrier, inc=1, device_id=(mate(k), t), device_id_type=MESH)
    for k in range(1, n_tp):
        pl.semaphore_signal(
            barrier, inc=1, device_id=(i, lax.rem(t + k, n_tp)), device_id_type=MESH
        )

    held = ((ids_h, ids), (wts_h, wts), (mix_h, mix), (og_h, og), (gb_h, gb), (st_h, st), (dc_h, dc))
    held = held + ((wg_h, wg), (wu_h, wu), (wd_h, wd), (wp_h, wp))
    loads = [pltpu.make_async_copy(a, b, w_sem.at[n]) for n, (a, b) in enumerate(held)]
    for load in loads:
        load.start()
    for load in loads[:4]:
        load.wait()

    with scope("build"):
        experts_iota = lax.broadcasted_iota(jnp.int32, (n_sp, tok), 0)
        named = jnp.zeros((n_sp, tok), F32)
        weight = jnp.zeros((n_sp, tok), F32)
        for k in range(ids.shape[0]):
            hit = ids[k : k + 1, :] == experts_iota
            named = jnp.where(hit, 1.0, named)
            weight = jnp.where(hit, wts[k : k + 1, :], weight)
        earlier = (
            lax.broadcasted_iota(jnp.int32, (tok, tok), 0)
            < lax.broadcasted_iota(jnp.int32, (tok, tok), 1)
        )
        place = dot(named.astype(BF16), jnp.where(earlier, 1.0, 0.0).astype(BF16), 1, 0)
        place = jnp.where(named > 0.5, place, -1.0).astype(jnp.int32)
        slot_iota = lax.broadcasted_iota(jnp.int32, (cap, tok), 0)
        for e in range(n_sp):
            here = jnp.where(place[e : e + 1, :] == slot_iota, 1.0, 0.0)
            slot_weight = jnp.sum(here * weight[e : e + 1, :], axis=1, keepdims=True)
            sel[e * cap : (e + 1) * cap, :] = here.astype(BF16)
            sw[e * cap : (e + 1) * cap, :] = jnp.broadcast_to(slot_weight, (cap, sw.shape[1]))
        chosen = sel[...]
        for q in range(ny):
            cols = columns(2 * y_up(q) + c)
            send[0, q] = dot(chosen, mix[:, cols], 1, 0).astype(BF16).reshape(n_sp, cap, dg)
            send[1, q] = (
                (dot(chosen, og[:, cols], 1, 0) * sw[:, 0:1]).astype(BF16).reshape(n_sp, cap, dg)
            )
    with scope("barrier"):
        pl.semaphore_wait(barrier, n_sp + n_tp - 2)

    pending = []

    def go(copy):
        copy.start()
        pending.append(copy)

    def groups(k):
        return range(ny) if k in straight else range(1)

    def dispatch(q, k):
        return remote(
            send.at[:, q, mate(k)],
            xc.at[:, 2 * y_up(q) + c, i],
            sp_s.at[q, k],
            sp_r.at[q, k],
            (mate(k), t),
        )

    for k in range(1, n_sp):
        for q in groups(k):
            go(dispatch(q, k))

    with scope("own"):
        mine = pl.ds(pl.multiple_of(i * cap, cap), cap)
        here, slot_weight = sel[mine, :], sw[mine, 0:1]
        for g in range(n_tp):
            cols = slice(g * dg, (g + 1) * dg)
            xc[0, g, i] = dot(here, mix[:, cols], 1, 0).astype(BF16)
            xc[1, g, i] = (dot(here, og[:, cols], 1, 0) * slot_weight).astype(BF16)
        for load in loads[4:7]:
            load.wait()
        ga[i] = (gb[...].astype(F32) * st[...]).astype(BF16)
    go(
        remote(
            st.at[pl.ds(tok - 8, 8)],
            pv,
            pv_sem.at[0],
            pv_sem.at[1],
            (lax.rem(i + 1, n_sp), t),
        )
    )
    pv_copy = pending[-1]

    def to_core(q, k):
        block = xc.at[:, 2 * y_up(q) + c, mate(k)]
        return remote(block, block, core_s.at[q, k], core_r.at[q, k], peer)

    def to_y(q, k):
        block = xc.at[:, t, mate(k)]
        return remote(block, block, y_s.at[q, k], y_r.at[q, k], (i, 2 * y_up(q) + c))

    def from_y(q, k):
        block = xc.at[:, 2 * y_up(ny - q) + c, mate(k)]
        return remote(block, block, y_s.at[q, k], y_r.at[q, k], (i, 2 * y_up(q) + c))

    def from_sp(q, k):
        return remote(
            send.at[:, q, mate(k)],
            xc.at[:, 2 * y_up(q) + c, mate(k)],
            sp_s.at[q, k],
            sp_r.at[q, k],
            (mate(k), t),
        )

    def from_core(q, k):
        block = xc.at[:, 2 * y_up(q) + 1 - c, mate(k)]
        return remote(block, block, core_s.at[q, k], core_r.at[q, k], peer)

    def chunk(m):
        return [k for k in range(*bounds[m]) if k]

    def rows_of_chunk(m):
        first, end = bounds[m]
        return pl.ds(first * cap, (end - first) * cap)

    def spread(ks):
        for k in ks:
            with scope(f"spread{k}"):
                for q in groups(k):
                    from_sp(q, k).wait_recv()
                if k not in straight:
                    for q in range(1, ny):
                        go(to_y(q, k))
                for q in groups(k):
                    go(to_core(q, k))

    def hand_on(ks):
        for k in ks:
            if k in straight:
                continue
            with scope(f"hand{k}"):
                for q in range(1, ny):
                    from_y(q, k).wait_recv()
                    go(to_core(ny - q, k))

    def arrived(m):
        with scope(f"arr{m}"):
            for k in chunk(m):
                for q in range(ny):
                    from_core(q, k).wait_recv()

    def expert(m):
        order = [mate(k) for k in range(*bounds[m])]

        def rows_of(which, g):
            return jnp.concatenate([xc[which, g, s] for s in order], axis=0)

        gate = up = hg = None
        for g in range(n_tp):
            cols = slice(g * dg, (g + 1) * dg)
            x, cot = rows_of(0, g), rows_of(1, g)
            parts = (dot(x, wg[:, cols], 1, 1), dot(x, wu[:, cols], 1, 1), dot(cot, wd[:, cols], 1, 1))
            if g == 0:
                gate, up, hg = parts
            else:
                gate, up, hg = gate + parts[0], up + parts[1], hg + parts[2]
        s = jax.nn.sigmoid(gate)
        silu = gate * s
        hidden = (silu * up).astype(BF16)
        up_grad = (hg * silu).astype(BF16)
        gate_grad = (hg * up * s * (1.0 + gate * (1.0 - s))).astype(BF16)
        for q, src in enumerate(order):
            part = slice(q * cap, (q + 1) * cap)
            hid[src] = hidden[part]
            ug[src] = up_grad[part]
            gg[src] = gate_grad[part]
        return gate_grad, up_grad

    def partial(gate_grad, up_grad, g):
        cols = columns(g)
        return (dot(gate_grad, wg[:, cols], 1, 0) + dot(up_grad, wu[:, cols], 1, 0)).astype(BF16)

    def swap_core(m, q):
        rows = rows_of_chunk(m)
        return remote(pb.at[q, rows], rc.at[q, rows], pc_s.at[m, q], pc_r.at[m, q], peer)

    def swap_y(m, q):
        rows = rows_of_chunk(m)
        return remote(
            qb.at[q, rows], ry.at[q, rows], py_s.at[m, q], py_r.at[m, q], (i, 2 * y_up(q) + c)
        )

    def run(m):
        arrived(m)
        with scope(f"exp{m}"):
            grads = expert(m)
        rows = rows_of_chunk(m)
        with scope(f"part{m}"):
            for q in list(range(1, ny)) + [0]:
                pb[q, rows] = partial(*grads, 2 * y_up(q) + 1 - c)
                go(swap_core(m, q))
            for q in list(range(1, ny)) + [0]:
                po[q, rows] = partial(*grads, 2 * y_up(q) + c)

    def fold_core(m):
        rows = rows_of_chunk(m)
        with scope(f"foldc{m}"):
            for q in range(1, ny):
                swap_core(m, q).wait_recv()
                qb[q, rows] = (po[q, rows].astype(F32) + rc[q, rows].astype(F32)).astype(BF16)
                go(swap_y(m, q))

    def home(k):
        return remote(
            fb.at[pl.ds(k * cap, cap)], ret.at[i], ret_s.at[k], ret_r.at[k], (mate(k), t)
        )

    def fold_y(m):
        rows = rows_of_chunk(m)
        with scope(f"foldy{m}"):
            swap_core(m, 0).wait_recv()
            total = po[0, rows].astype(F32) + rc[0, rows].astype(F32)
            for q in range(1, ny):
                swap_y(m, q).wait_recv()
                total = total + ry[q, rows].astype(F32)
            total = total.astype(BF16)
            fb[rows] = total
            if m == 0:
                ret[i] = total[:cap]
            for k in chunk(m):
                go(home(k))

    def weight_grad(left, which, out):
        with scope("wgrad"):
            a = left[...].reshape(slots, left.shape[2])
            for g in range(n_tp):
                b = xc[which, g].reshape(slots, dg)
                out[:, g * dg : (g + 1) * dg] = dot(a, b, 0, 0).astype(BF16)

    def share_gated(k):
        return remote(ga.at[i], ga.at[i], ga_s.at[k], ga_r.at[k], (mate(k), t))

    def get_gated(k):
        return remote(ga.at[i], ga.at[mate(k)], ga_s.at[k], ga_r.at[k], (mate(k), t))

    def pass_gated(k):
        block = ga.at[mate(k)]
        return remote(block, block, ga_s.at[k + 1], ga_r.at[k + 1], (mate(1), t))

    def passed_gated(k):
        block = ga.at[mate(k + 1)]
        return remote(block, block, ga_s.at[k + 1], ga_r.at[k + 1], (mate(1), t))

    far = [k for k in range(2, n_sp, 2)]

    near = chunk(0)
    spread(near[1:])
    spread(near[:1])
    spread(chunk(1))
    hand_on(chunk(0))
    for load in loads[7:]:
        load.wait()
    run(0)
    spread(chunk(2))
    fold_core(0)
    for k in far:
        go(share_gated(k))
    hand_on(chunk(1))
    run(1)
    fold_core(1)
    hand_on(chunk(2))
    fold_y(0)
    run(2)
    fold_core(2)
    fold_y(1)
    weight_grad(gg, 0, dwg)
    fold_y(2)
    weight_grad(ug, 0, dwu)
    weight_grad(hid, 1, dwd)
    with scope("gated"):
        for k in range(0, n_sp, 2):
            if k:
                get_gated(k).wait_recv()
            go(pass_gated(k))

    def from_expert(k):
        return remote(
            fb.at[pl.ds(k * cap, cap)],
            ret.at[mate(k)],
            ret_s.at[k],
            ret_r.at[k],
            (mate(k), t),
        )

    for k in range(1, n_sp):
        with scope(f"ret{k}"):
            from_expert(k).wait_recv()
    with scope("mid"):
        routed = dot(ret[...].reshape(slots, dg), sel[...], 0, 0)
        mid = (og[:, columns(t)].astype(F32).T + routed).astype(BF16)
        mt[t] = mid

    def mid_core(q):
        block = mt.at[2 * y_up(q) + c]
        return remote(block, block, mtc_s.at[q], mtc_r.at[q], peer)

    def mid_from_core(q):
        block = mt.at[2 * y_up(q) + 1 - c]
        return remote(block, block, mtc_s.at[q], mtc_r.at[q], peer)

    def mid_y(q):
        return remote(mt.at[t], mt.at[t], mty_s.at[q], mty_r.at[q], (i, 2 * y_up(q) + c))

    def mid_from_y(q):
        block = mt.at[2 * y_up(ny - q) + c]
        return remote(block, block, mty_s.at[q], mty_r.at[q], (i, 2 * y_up(q) + c))

    for q in range(1, ny):
        go(mid_y(q))
    go(mid_core(0))

    row = lax.broadcasted_iota(jnp.int32, dc.shape, 0)
    decay = dc[...]
    head = decay[0:1, :]
    factor = jnp.where(row < tok - 1, pltpu.roll(decay, tok - 1, 0), 1.0)
    with scope("midx"):
        for q in range(1, ny):
            mid_from_y(q).wait_recv()
            go(mid_core(ny - q))
        for q in range(ny):
            mid_from_core(q).wait_recv()

    share = 2 * mr.shape[2]
    per = dg // share if dg >= share else 1

    part = share // 2

    def rows_for(s, h):
        first = (s % per) * share + h * part
        return mt.at[s // per, pl.ds(pl.multiple_of(first, part), part)]

    def share_rows(k):
        return remote(rows_for(mate(k), c), mr.at[i, c], mr_s.at[k], mr_r.at[k], (mate(k), t))

    def get_rows(k):
        return remote(
            rows_for(mate(k), c), mr.at[mate(k), c], mr_s.at[k], mr_r.at[k], (mate(k), t)
        )

    def swap_rows(k, h):
        block = mr.at[mate(k), h]
        return remote(block, block, mrc_s.at[k], mrc_r.at[k], peer)

    for k in range(n_sp - 1, 0, -1):
        go(share_rows(k))

    with scope("scan"):
        act = dot(mt[...].reshape(n_tp * dg, tok), wp[...], 0, 0)
        grad = act * gb[...].astype(F32)
        gbr[...] = (act * st[...]).astype(BF16)
        step = 1
        while step < tok:
            inside = row < tok - step
            grad = grad + jnp.where(inside, factor * pltpu.roll(grad, tok - step, 0), 0.0)
            factor = factor * jnp.where(inside, pltpu.roll(factor, tok - step, 0), 1.0)
            step *= 2
        pair = jnp.concatenate([head * factor[0:1, :], head * grad[0:1, :]], axis=0)
        pair = jnp.concatenate([pair, jnp.zeros((6, pair.shape[1]), F32)], axis=0)
        cs[...] = pair
        cr[i] = pair

    def share_carry(k):
        return remote(cs, cr.at[i], c_s.at[k], c_r.at[k], (mate(k), t))

    def get_carry(k):
        return remote(cs, cr.at[mate(k)], c_s.at[k], c_r.at[k], (mate(k), t))

    for k in range(1, n_sp):
        go(share_carry(k))
    for h in range(2):
        mr[i, h] = rows_for(i, h)[...]

    for k in range(1, n_sp):
        with scope(f"rows{k}"):
            get_rows(k).wait_recv()
            go(swap_rows(k, c))
    with scope("passed"):
        for k in range(0, n_sp, 2):
            passed_gated(k).wait_recv()
    with scope("gproj"):
        total = None
        for k in range(n_sp):
            if k:
                swap_rows(k, 1 - c).wait_recv()
            src = mate(k)
            term = dot(mr[src].reshape(share, tok), ga[src], 1, 0)
            total = term if total is None else total + term
        gproj[...] = total

    with scope("carry"):
        for k in range(1, n_sp):
            get_carry(k).wait_recv()
        carry = jnp.zeros((1, pair.shape[1]), F32)
        for s in range(n_sp - 1, 0, -1):
            carry = jnp.where(s > i, cr[s, 1:2, :] + cr[s, 0:1, :] * carry, carry)
        drive = grad + factor * carry
        gdr[...] = drive
        pv_copy.wait_recv()
        states = st[...]
        last = jnp.where(i > 0, pv[7:8, :], 0.0)
        previous = jnp.where(row == 0, last, pltpu.roll(states, 1, 0))
        gdc[...] = drive * previous

    with scope("drain"):
        for copy in pending:
            copy.wait_send()


def settle(count, *refs):
    ins, outs, sem = refs[:count], refs[count : 2 * count], refs[2 * count]
    puts = [pltpu.make_async_copy(ins[n], outs[n], sem.at[n]) for n in range(count)]
    for put in puts:
        put.start()
    for put in puts:
        put.wait()


def local(
    mixer_out,
    out_grad,
    route_ids,
    route_weights,
    gate_branch,
    states,
    decay,
    w_proj,
    w_gate,
    w_up,
    w_down,
):
    tok, width = mixer_out.shape
    top = route_ids.shape[1]
    n_sp, n_tp = lax.axis_size("sp"), lax.axis_size("tp")
    ny = n_tp // 2
    assert w_gate.shape[0] == 1
    cap = 2 * top * tok // n_sp
    dg = width // n_tp
    hidden = w_gate.shape[1]
    channels = states.shape[1]
    share = width // n_sp
    vmem = pl.BlockSpec(memory_space=pltpu.VMEM)
    hbm = pl.BlockSpec(memory_space=pltpu.HBM)
    dma = pltpu.SemaphoreType.DMA
    weight = (hidden, width)
    outs = pl.pallas_call(
        functools.partial(kernel, n_sp, n_tp),
        out_shape=[jax.ShapeDtypeStruct(weight, BF16)] * 3
        + [
            jax.ShapeDtypeStruct((share, channels), F32),
            jax.ShapeDtypeStruct((tok, channels), BF16),
            jax.ShapeDtypeStruct((tok, channels), F32),
            jax.ShapeDtypeStruct((tok, channels), F32),
        ],
        in_specs=[hbm] * 11,
        out_specs=[vmem] * 7,
        scratch_shapes=[
            pltpu.VMEM((top, tok), jnp.int32),
            pltpu.VMEM((top, tok), F32),
            pltpu.VMEM((tok, width), BF16),
            pltpu.VMEM((tok, width), BF16),
            pltpu.VMEM((tok, channels), BF16),
            pltpu.VMEM((tok, channels), F32),
            pltpu.VMEM((tok, channels), F32),
            pltpu.VMEM((width, channels), BF16),
            *([pltpu.VMEM(weight, BF16)] * 3),
            pltpu.VMEM((n_sp * cap, tok), BF16),
            pltpu.VMEM((n_sp * cap, 128), F32),
            pltpu.VMEM((2, ny, n_sp, cap, dg), BF16),
            pltpu.VMEM((2, n_tp, n_sp, cap, dg), BF16),
            pltpu.VMEM((n_sp, tok, channels), BF16),
            pltpu.VMEM((8, channels), F32),
            *([pltpu.VMEM((n_sp, cap, hidden), BF16)] * 3),
            *([pltpu.VMEM((ny, n_sp * cap, dg), BF16)] * 5),
            pltpu.VMEM((n_sp * cap, dg), BF16),
            pltpu.VMEM((n_sp, cap, dg), BF16),
            pltpu.VMEM((n_tp, dg, tok), BF16),
            pltpu.VMEM((n_sp, 2, share // 2, tok), BF16),
            pltpu.VMEM((8, channels), F32),
            pltpu.VMEM((n_sp, 8, channels), F32),
            dma((11,)),
            *([dma((ny, n_sp))] * 6),
            dma((n_sp,)),
            dma((n_sp,)),
            dma((2,)),
            *([dma((3, ny))] * 4),
            dma((n_sp,)),
            dma((n_sp,)),
            *([dma((ny,))] * 4),
            *([dma((n_sp,))] * 6),
        ],
        compiler_params=pltpu.CompilerParams(
            collective_id=0, has_side_effects=True, vmem_limit_bytes=LIMIT
        ),
    )(
        *(
            pltpu.with_memory_space_constraint(x, pltpu.HBM)
            for x in (
                route_ids.T,
                route_weights.T,
                mixer_out,
                out_grad,
                gate_branch,
                states,
                decay,
                w_proj,
                w_gate[0],
                w_up[0],
                w_down[0],
            )
        )
    )
    count = len(outs)
    outs = pl.pallas_call(
        functools.partial(settle, count),
        out_shape=[jax.ShapeDtypeStruct(o.shape, o.dtype) for o in outs],
        in_specs=[vmem] * count,
        out_specs=[hbm] * count,
        scratch_shapes=[dma((count,))],
        compiler_params=pltpu.CompilerParams(vmem_limit_bytes=LIMIT),
    )(*outs)
    return (outs[0][None], outs[1][None], outs[2][None], *outs[3:])


def solution(mesh):
    placed = (
        P("sp", None),
        P("sp", None),
        P("sp", None),
        P("sp", None),
        P("sp", "tp"),
        P("sp", "tp"),
        P("sp", "tp"),
        P(None, "tp"),
        P("sp", "tp", None),
        P("sp", "tp", None),
        P("sp", "tp", None),
    )
    return jax.shard_map(
        local,
        mesh=mesh,
        in_specs=placed,
        out_specs=(
            P("sp", "tp", None),
            P("sp", "tp", None),
            P("sp", "tp", None),
            P("sp", "tp"),
            P("sp", "tp"),
            P("sp", "tp"),
            P("sp", "tp"),
        ),
        check_vma=False,
    )
```

```python
import functools

import jax
import jax.numpy as jnp
from jax import lax
from jax.experimental import pallas as pl
from jax.experimental.pallas import tpu as pltpu
from jax.sharding import PartitionSpec as P

MESH = pl.DeviceIdType.MESH
F32 = jnp.float32
BF16 = jnp.bfloat16
LIMIT = 44 * 1024 * 1024


def dot(a, b, ca, cb):
    return lax.dot_general(a, b, (((ca,), (cb,)), ((), ())), preferred_element_type=F32)


def kernel(
    n_sp,
    n_tp,
    ids_h,
    wts_h,
    mix_h,
    og_h,
    gb_h,
    st_h,
    dc_h,
    wp_h,
    wg_h,
    wu_h,
    wd_h,
    dwg,
    dwu,
    dwd,
    gproj,
    gbr,
    gdr,
    gdc,
    ids,
    wts,
    mix,
    og,
    gb,
    st,
    dc,
    wp,
    wg,
    wu,
    wd,
    sel,
    sw,
    send,
    xc,
    ga,
    pv,
    gg,
    ug,
    hid,
    pb,
    po,
    rc,
    qb,
    ry,
    fb,
    ret,
    mt,
    mr,
    cs,
    cr,
    w_sem,
    put,
    one_r,
    sp_r,
    core_r,
    y_r,
    pc_r,
    py_r,
    mty_r,
    mr_r,
):
    i = lax.axis_index("sp")
    t = lax.axis_index("tp")
    ny = n_tp // 2
    y, c = t // 2, t % 2
    tok = mix.shape[0]
    cap = xc.shape[3]
    dg = xc.shape[4]
    slots = n_sp * cap
    peer = (i, y * 2 + 1 - c)
    straight = (1,)
    quarter = n_sp // 4
    bounds = ((0, n_sp // 2), (n_sp // 2, 3 * n_sp // 4), (3 * n_sp // 4, n_sp))
    pieces = ((0, 1), (2,), (3,))
    scope = jax.named_scope

    def columns(g):
        return pl.ds(pl.multiple_of(g * dg, dg), dg)

    def mate(k):
        to, bit = i, 1
        while bit <= k:
            if k & bit:
                to = to + bit * (1 - 2 * ((i // bit) % 2))
            bit *= 2
        return to

    def y_up(q):
        return lax.rem(y + q, ny)

    def remote(src, dst, s, r, who):
        return pltpu.make_async_remote_copy(
            src_ref=src, dst_ref=dst, send_sem=s, recv_sem=r, device_id=who, device_id_type=MESH
        )

    def took(ref, sem):
        remote(ref, ref, sem, sem, peer).wait_recv()

    barrier = pltpu.get_barrier_semaphore()
    for k in range(1, n_sp):
        pl.semaphore_signal(barrier, inc=1, device_id=(mate(k), t), device_id_type=MESH)
    for k in range(1, n_tp):
        pl.semaphore_signal(
            barrier, inc=1, device_id=(i, lax.rem(t + k, n_tp)), device_id_type=MESH
        )

    held = ((ids_h, ids), (wts_h, wts), (mix_h, mix), (og_h, og), (gb_h, gb), (st_h, st), (dc_h, dc))
    held = held + ((wg_h, wg), (wu_h, wu), (wd_h, wd), (wp_h, wp))
    loads = [pltpu.make_async_copy(a, b, w_sem.at[n]) for n, (a, b) in enumerate(held)]
    for load in loads:
        load.start()
    for load in loads[:4]:
        load.wait()

    with scope("build"):
        experts_iota = lax.broadcasted_iota(jnp.int32, (n_sp, tok), 0)
        named = jnp.zeros((n_sp, tok), F32)
        weight = jnp.zeros((n_sp, tok), F32)
        for k in range(ids.shape[0]):
            hit = ids[k : k + 1, :] == experts_iota
            named = jnp.where(hit, 1.0, named)
            weight = jnp.where(hit, wts[k : k + 1, :], weight)
        earlier = (
            lax.broadcasted_iota(jnp.int32, (tok, tok), 0)
            < lax.broadcasted_iota(jnp.int32, (tok, tok), 1)
        )
        place = dot(named.astype(BF16), jnp.where(earlier, 1.0, 0.0).astype(BF16), 1, 0)
        place = jnp.where(named > 0.5, place, -1.0).astype(jnp.int32)
        slot_iota = lax.broadcasted_iota(jnp.int32, (cap, tok), 0)
        for e in range(n_sp):
            here = jnp.where(place[e : e + 1, :] == slot_iota, 1.0, 0.0)
            slot_weight = jnp.sum(here * weight[e : e + 1, :], axis=1, keepdims=True)
            sel[e * cap : (e + 1) * cap, :] = here.astype(BF16)
            sw[e * cap : (e + 1) * cap, :] = jnp.broadcast_to(slot_weight, (cap, sw.shape[1]))
        chosen = sel[...]
        for q in range(ny):
            cols = columns(2 * y_up(q) + c)
            send[0, q] = dot(chosen, mix[:, cols], 1, 0).astype(BF16).reshape(n_sp, cap, dg)
            send[1, q] = (
                (dot(chosen, og[:, cols], 1, 0) * sw[:, 0:1]).astype(BF16).reshape(n_sp, cap, dg)
            )
    with scope("barrier"):
        pl.semaphore_wait(barrier, n_sp + n_tp - 2)

    def groups(k):
        return range(ny) if k in straight else range(1)

    def dispatch(q, k):
        return remote(
            send.at[:, q, mate(k)],
            xc.at[:, 2 * y_up(q) + c, i],
            put.at[0 if q == 0 else 1],
            sp_r.at[k if q == 0 else n_sp + q - 1],
            (mate(k), t),
        )

    for k in range(1, n_sp):
        for q in groups(k):
            dispatch(q, k).start()

    with scope("own"):
        mine = pl.ds(pl.multiple_of(i * cap, cap), cap)
        here, slot_weight = sel[mine, :], sw[mine, 0:1]
        for g in range(n_tp):
            cols = slice(g * dg, (g + 1) * dg)
            xc[0, g, i] = dot(here, mix[:, cols], 1, 0).astype(BF16)
            xc[1, g, i] = (dot(here, og[:, cols], 1, 0) * slot_weight).astype(BF16)
        for load in loads[4:7]:
            load.wait()
        ga[i] = (gb[...].astype(F32) * st[...]).astype(BF16)
    pv_copy = remote(
        st.at[pl.ds(tok - 8, 8)], pv, put.at[2], one_r.at[0], (lax.rem(i + 1, n_sp), t)
    )
    pv_copy.start()

    def chunk_of(k):
        return [first <= k < end for first, end in bounds].index(True)

    def to_core(q, k):
        block = xc.at[:, 2 * y_up(q) + c, mate(k)]
        return remote(block, block, put.at[3], core_r.at[chunk_of(k)], peer)

    def to_y(q, k):
        block = xc.at[:, t, mate(k)]
        return remote(block, block, put.at[4], y_r.at[q - 1, k], (i, 2 * y_up(q) + c))

    def from_y(q, k):
        block = xc.at[:, 2 * y_up(ny - q) + c, mate(k)]
        took(block, y_r.at[q - 1, k])

    def from_sp(q, k):
        took(xc.at[:, 2 * y_up(q) + c, mate(k)], sp_r.at[k if q == 0 else n_sp + q - 1])

    def chunk(m):
        return [k for k in range(*bounds[m]) if k]

    def piece(p):
        return range(p * quarter, (p + 1) * quarter)

    def rows_of(p):
        return pl.ds(p * quarter * cap, quarter * cap)

    def spread(ks):
        for k in ks:
            with scope(f"spread{k}"):
                for q in groups(k):
                    from_sp(q, k)
                if k not in straight:
                    for q in range(1, ny):
                        to_y(q, k).start()
                for q in groups(k):
                    to_core(q, k).start()

    def hand_on(ks):
        for k in ks:
            if k in straight:
                continue
            with scope(f"hand{k}"):
                for q in range(1, ny):
                    from_y(q, k)
                    to_core(ny - q, k).start()

    def arrived(m):
        with scope(f"arr{m}"):
            took(xc.at[:, :ny, : len(chunk(m))], core_r.at[m])

    def expert(m):
        order = [mate(k) for k in range(*bounds[m])]

        def gathered(which, g):
            return jnp.concatenate([xc[which, g, s] for s in order], axis=0)

        gate = up = hg = None
        for g in range(n_tp):
            cols = slice(g * dg, (g + 1) * dg)
            x, cot = gathered(0, g), gathered(1, g)
            parts = (dot(x, wg[:, cols], 1, 1), dot(x, wu[:, cols], 1, 1), dot(cot, wd[:, cols], 1, 1))
            if g == 0:
                gate, up, hg = parts
            else:
                gate, up, hg = gate + parts[0], up + parts[1], hg + parts[2]
        s = jax.nn.sigmoid(gate)
        silu = gate * s
        hidden = (silu * up).astype(BF16)
        up_grad = (hg * silu).astype(BF16)
        gate_grad = (hg * up * s * (1.0 + gate * (1.0 - s))).astype(BF16)
        for q, src in enumerate(order):
            part = slice(q * cap, (q + 1) * cap)
            hid[src] = hidden[part]
            ug[src] = up_grad[part]
            gg[src] = gate_grad[part]
        return gate_grad, up_grad

    def partial(gate_grad, up_grad, g):
        cols = columns(g)
        return (dot(gate_grad, wg[:, cols], 1, 0) + dot(up_grad, wu[:, cols], 1, 0)).astype(BF16)

    def swap_core(p, q):
        rows = rows_of(p)
        return remote(pb.at[q, rows], rc.at[q, rows], put.at[5], pc_r.at[p, q], peer)

    def swap_y(p, q):
        rows = rows_of(p)
        return remote(
            qb.at[q, rows], ry.at[q, rows], put.at[6], py_r.at[p, q - 1], (i, 2 * y_up(q) + c)
        )

    def run(m):
        arrived(m)
        with scope(f"exp{m}"):
            grads = expert(m)
        rows = pl.ds(bounds[m][0] * cap, (bounds[m][1] - bounds[m][0]) * cap)
        with scope(f"part{m}"):
            for q in list(range(1, ny)) + [0]:
                pb[q, rows] = partial(*grads, 2 * y_up(q) + 1 - c)
                for p in reversed(pieces[m]):
                    swap_core(p, q).start()
            for q in list(range(1, ny)) + [0]:
                po[q, rows] = partial(*grads, 2 * y_up(q) + c)

    def fold_core(p):
        rows = rows_of(p)
        with scope(f"foldc{p}"):
            for q in range(1, ny):
                took(rc.at[q, rows], pc_r.at[p, q])
                qb[q, rows] = (po[q, rows].astype(F32) + rc[q, rows].astype(F32)).astype(BF16)
                swap_y(p, q).start()

    def home(k):
        return remote(
            fb.at[pl.ds(k * cap, cap)], ret.at[i], put.at[7], one_r.at[1], (mate(k), t)
        )

    def fold_y(p):
        rows = rows_of(p)
        with scope(f"foldy{p}"):
            took(rc.at[0, rows], pc_r.at[p, 0])
            total = po[0, rows].astype(F32) + rc[0, rows].astype(F32)
            for q in range(1, ny):
                took(ry.at[q, rows], py_r.at[p, q - 1])
                total = total + ry[q, rows].astype(F32)
            total = total.astype(BF16)
            fb[rows] = total
            if p == 0:
                ret[i] = total[:cap]
            for k in piece(p):
                if k:
                    home(k).start()

    def weight_grad(left, which, out):
        with scope("wgrad"):
            a = left[...].reshape(slots, left.shape[2])
            for g in range(n_tp):
                b = xc[which, g].reshape(slots, dg)
                out[:, g * dg : (g + 1) * dg] = dot(a, b, 0, 0).astype(BF16)

    def share_gated(k):
        return remote(ga.at[i], ga.at[i], put.at[8], one_r.at[2], (mate(k), t))

    def pass_gated(k):
        block = ga.at[mate(k)]
        return remote(block, block, put.at[8], one_r.at[3], (mate(1), t))

    far = [k for k in range(2, n_sp, 2)]

    near = chunk(0)
    spread(near[1:])
    spread(near[:1])
    spread(chunk(1))
    hand_on(chunk(0))
    for load in loads[7:]:
        load.wait()
    run(0)
    spread(chunk(2))
    fold_core(1)
    for k in far:
        share_gated(k).start()
    hand_on(chunk(1))
    run(1)
    fold_core(2)
    fold_core(0)
    hand_on(chunk(2))
    run(2)
    fold_core(3)
    fold_y(1)
    fold_y(2)
    fold_y(0)
    weight_grad(gg, 0, dwg)
    fold_y(3)
    weight_grad(ug, 0, dwu)
    weight_grad(hid, 1, dwd)
    with scope("gated"):
        took(ga.at[pl.ds(0, len(far))], one_r.at[2])
        for k in range(0, n_sp, 2):
            pass_gated(k).start()

    with scope("ret"):
        took(ret.at[pl.ds(1, n_sp - 1)], one_r.at[1])
    with scope("mid"):
        routed = dot(ret[...].reshape(slots, dg), sel[...], 0, 0)
        mid = (og[:, columns(t)].astype(F32).T + routed).astype(BF16)
        mt[t] = mid

    def mid_core(q):
        block = mt.at[2 * y_up(q) + c]
        return remote(block, block, put.at[9], one_r.at[4], peer)

    def mid_y(q):
        return remote(mt.at[t], mt.at[t], put.at[9], mty_r.at[q - 1], (i, 2 * y_up(q) + c))

    for q in range(1, ny):
        mid_y(q).start()
    mid_core(0).start()

    part = mr.shape[2]
    share = 2 * part
    per = dg // share
    others = [(1, n_sp // 2), (n_sp // 2, 3 * n_sp // 4), (3 * n_sp // 4, n_sp)]

    def share_rows(k):
        s = mate(k)
        first = pl.multiple_of((s % per) * share + c * part, part)
        group = [first <= k < end for first, end in others].index(True)
        return remote(
            mt.at[s // per, pl.ds(first, part)], mr.at[k, c], put.at[10], mr_r.at[group], (s, t)
        )

    def pass_rows(n):
        with scope(f"rows{n}"):
            first, end = others[n]
            block = mr.at[pl.ds(first, end - first), c]
            took(block, mr_r.at[n])
            remote(block, block, put.at[11], one_r.at[6], peer).start()

    width = dc.shape[1]
    row = lax.broadcasted_iota(jnp.int32, dc.shape, 0)
    decay = dc[...]
    head = decay[0:1, :]
    factor = jnp.where(row < tok - 1, pltpu.roll(decay, tok - 1, 0), 1.0)
    with scope("midx"):
        for q in range(1, ny):
            took(mt.at[2 * y_up(ny - q) + c], mty_r.at[q - 1])
            mid_core(ny - q).start()

    with scope("midc"):
        took(mt.at[pl.ds(0, ny)], one_r.at[4])
    for k in range(n_sp - 1, 0, -1):
        share_rows(k).start()

    with scope("scan"):
        act = dot(mt[...].reshape(n_tp * dg, tok), wp[...], 0, 0)
        grad = act * gb[...].astype(F32)
        gbr[...] = (act * st[...]).astype(BF16)
        step = 1
        while step < tok:
            inside = row < tok - step
            grad = grad + jnp.where(inside, factor * pltpu.roll(grad, tok - step, 0), 0.0)
            factor = factor * jnp.where(inside, pltpu.roll(factor, tok - step, 0), 1.0)
            step *= 2
        cs[...] = jnp.zeros(cs.shape, F32)
        for j in range(width // 128):
            lanes = slice(j * 128, (j + 1) * 128)
            cs[j : j + 1, :] = head[:, lanes] * factor[0:1, lanes]
            cs[width // 128 + j : width // 128 + j + 1, :] = head[:, lanes] * grad[0:1, lanes]

    def share_carry(k):
        return remote(cs, cr.at[i], put.at[12], one_r.at[5], (mate(k), t))

    for k in range(n_sp - 1, 0, -1):
        share_carry(k).start()

    for n in range(3):
        pass_rows(n)
    with scope("passed"):
        took(ga.at[pl.ds(0, n_sp // 2)], one_r.at[3])
    with scope("gproj0"):
        own = mt[i // per, pl.ds(pl.multiple_of((i % per) * share, share), share)]
        total = dot(own, ga[i], 1, 0)
    with scope("rowsc"):
        took(mr.at[pl.ds(1, n_sp - 1), 0], one_r.at[6])
    with scope("gproj"):
        for k in range(1, n_sp):
            total = total + dot(mr[k].reshape(share, tok), ga[mate(k)], 1, 0)
        gproj[...] = total

    with scope("carry"):
        took(cr.at[pl.ds(1, n_sp - 1)], one_r.at[5])

        def lane_row(s, first):
            return jnp.concatenate(
                [cr[s, first + j : first + j + 1, :] for j in range(width // 128)], axis=1
            )

        carry = jnp.zeros((1, width), F32)
        for s in range(n_sp - 1, 0, -1):
            carry = jnp.where(s > i, lane_row(s, width // 128) + lane_row(s, 0) * carry, carry)
        drive = grad + factor * carry
        gdr[...] = drive
        pv_copy.wait_recv()
        states = st[...]
        last = jnp.where(i > 0, pv[7:8, :], 0.0)
        previous = jnp.where(row == 0, last, pltpu.roll(states, 1, 0))
        gdc[...] = drive * previous

    with scope("drain"):
        took(xc.at[:, 0, pl.ds(1, n_sp - 1)], put.at[0])
        took(xc.at[:, pl.ds(0, ny - 1), 0], put.at[1])
        pv_copy.wait_send()
        took(xc.at[:, pl.ds(0, ny), pl.ds(1, n_sp - 1)], put.at[3])
        took(xc.at[:, pl.ds(0, ny - 1), pl.ds(2, n_sp - 2)], put.at[4])
        took(pb, put.at[5])
        took(qb.at[pl.ds(1, ny - 1)], put.at[6])
        took(fb.at[pl.ds(cap, (n_sp - 1) * cap)], put.at[7])
        took(ga.at[pl.ds(1, n_sp - 1)], put.at[8])
        took(mt.at[pl.ds(1, n_tp - 1)], put.at[9])
        took(mr.at[pl.ds(1, n_sp - 1), 0], put.at[10])
        took(mr.at[pl.ds(1, n_sp - 1), 0], put.at[11])
        took(cr.at[pl.ds(1, n_sp - 1)], put.at[12])


def settle(count, *refs):
    ins, outs, sem = refs[:count], refs[count : 2 * count], refs[2 * count]
    puts = [pltpu.make_async_copy(ins[n], outs[n], sem.at[n]) for n in range(count)]
    for put in puts:
        put.start()
    for put in puts:
        put.wait()


def local(
    mixer_out,
    out_grad,
    route_ids,
    route_weights,
    gate_branch,
    states,
    decay,
    w_proj,
    w_gate,
    w_up,
    w_down,
):
    tok, width = mixer_out.shape
    top = route_ids.shape[1]
    n_sp, n_tp = lax.axis_size("sp"), lax.axis_size("tp")
    ny = n_tp // 2
    assert w_gate.shape[0] == 1
    cap = 2 * top * tok // n_sp
    dg = width // n_tp
    hidden = w_gate.shape[1]
    channels = states.shape[1]
    share = width // n_sp
    vmem = pl.BlockSpec(memory_space=pltpu.VMEM)
    hbm = pl.BlockSpec(memory_space=pltpu.HBM)
    dma = pltpu.SemaphoreType.DMA
    weight = (hidden, width)
    outs = pl.pallas_call(
        functools.partial(kernel, n_sp, n_tp),
        out_shape=[jax.ShapeDtypeStruct(weight, BF16)] * 3
        + [
            jax.ShapeDtypeStruct((share, channels), F32),
            jax.ShapeDtypeStruct((tok, channels), BF16),
            jax.ShapeDtypeStruct((tok, channels), F32),
            jax.ShapeDtypeStruct((tok, channels), F32),
        ],
        in_specs=[hbm] * 11,
        out_specs=[vmem] * 7,
        scratch_shapes=[
            pltpu.VMEM((top, tok), jnp.int32),
            pltpu.VMEM((top, tok), F32),
            pltpu.VMEM((tok, width), BF16),
            pltpu.VMEM((tok, width), BF16),
            pltpu.VMEM((tok, channels), BF16),
            pltpu.VMEM((tok, channels), F32),
            pltpu.VMEM((tok, channels), F32),
            pltpu.VMEM((width, channels), BF16),
            *([pltpu.VMEM(weight, BF16)] * 3),
            pltpu.VMEM((n_sp * cap, tok), BF16),
            pltpu.VMEM((n_sp * cap, 128), F32),
            pltpu.VMEM((2, ny, n_sp, cap, dg), BF16),
            pltpu.VMEM((2, n_tp, n_sp, cap, dg), BF16),
            pltpu.VMEM((n_sp, tok, channels), BF16),
            pltpu.VMEM((8, channels), F32),
            *([pltpu.VMEM((n_sp, cap, hidden), BF16)] * 3),
            *([pltpu.VMEM((ny, n_sp * cap, dg), BF16)] * 5),
            pltpu.VMEM((n_sp * cap, dg), BF16),
            pltpu.VMEM((n_sp, cap, dg), BF16),
            pltpu.VMEM((n_tp, dg, tok), BF16),
            pltpu.VMEM((n_sp, 2, share // 2, tok), BF16),
            pltpu.VMEM((max(8, channels // 64), 128), F32),
            pltpu.VMEM((n_sp, max(8, channels // 64), 128), F32),
            dma((11,)),
            dma((13,)),
            dma((7,)),
            dma((n_sp + ny - 1,)),
            dma((3,)),
            dma((ny - 1, n_sp)),
            dma((4, ny)),
            dma((4, ny - 1)),
            dma((ny - 1,)),
            dma((3,)),
        ],
        compiler_params=pltpu.CompilerParams(
            collective_id=0, has_side_effects=True, vmem_limit_bytes=LIMIT
        ),
    )(
        *(
            pltpu.with_memory_space_constraint(x, pltpu.HBM)
            for x in (
                route_ids.T,
                route_weights.T,
                mixer_out,
                out_grad,
                gate_branch,
                states,
                decay,
                w_proj,
                w_gate[0],
                w_up[0],
                w_down[0],
            )
        )
    )
    count = len(outs)
    outs = pl.pallas_call(
        functools.partial(settle, count),
        out_shape=[jax.ShapeDtypeStruct(o.shape, o.dtype) for o in outs],
        in_specs=[vmem] * count,
        out_specs=[hbm] * count,
        scratch_shapes=[dma((count,))],
        compiler_params=pltpu.CompilerParams(vmem_limit_bytes=LIMIT),
    )(*outs)
    return (outs[0][None], outs[1][None], outs[2][None], *outs[3:])


def solution(mesh):
    placed = (
        P("sp", None),
        P("sp", None),
        P("sp", None),
        P("sp", None),
        P("sp", "tp"),
        P("sp", "tp"),
        P("sp", "tp"),
        P(None, "tp"),
        P("sp", "tp", None),
        P("sp", "tp", None),
        P("sp", "tp", None),
    )
    return jax.shard_map(
        local,
        mesh=mesh,
        in_specs=placed,
        out_specs=(
            P("sp", "tp", None),
            P("sp", "tp", None),
            P("sp", "tp", None),
            P("sp", "tp"),
            P("sp", "tp"),
            P("sp", "tp"),
            P("sp", "tp"),
        ),
        check_vma=False,
    )
```

```python
import functools

import jax
import jax.numpy as jnp
from jax import lax
from jax.experimental import pallas as pl
from jax.experimental.pallas import tpu as pltpu
from jax.sharding import PartitionSpec as P

MESH = pl.DeviceIdType.MESH
F32 = jnp.float32
BF16 = jnp.bfloat16
STRAIGHT = (1, 3)
LIMIT = 44 * 1024 * 1024


def dot(a, b, ca, cb):
    return lax.dot_general(a, b, (((ca,), (cb,)), ((), ())), preferred_element_type=F32)


def kernel(
    n_sp,
    n_tp,
    ids_h,
    wts_h,
    mix_h,
    og_h,
    gb_h,
    st_h,
    dc_h,
    wp_h,
    wg_h,
    wu_h,
    wd_h,
    dwg,
    dwu,
    dwd,
    gproj,
    gbr,
    gdr,
    gdc,
    ids,
    wts,
    mix,
    og,
    gb,
    st,
    dc,
    wp,
    wg,
    wu,
    wd,
    sel,
    sw,
    send,
    xc,
    ga,
    pv,
    gg,
    ug,
    hid,
    pb,
    po,
    rc,
    qb,
    ry,
    fb,
    ret,
    mt,
    mr,
    cs,
    cr,
    w_sem,
    put,
    one_r,
    sp_r,
    core_r,
    y_r,
    pc_r,
    py_r,
    mty_r,
    mr_r,
    ga_r,
):
    i = lax.axis_index("sp")
    t = lax.axis_index("tp")
    ny = n_tp // 2
    y, c = t // 2, t % 2
    tok = mix.shape[0]
    cap = xc.shape[3]
    dg = xc.shape[4]
    slots = n_sp * cap
    peer = (i, y * 2 + 1 - c)
    straight = STRAIGHT
    quarter = n_sp // 4
    bounds = ((0, n_sp // 2), (n_sp // 2, 3 * n_sp // 4), (3 * n_sp // 4, n_sp))
    pieces = ((0, 1), (2,), (3,))
    scope = jax.named_scope

    def columns(g):
        return pl.ds(pl.multiple_of(g * dg, dg), dg)

    def mate(k):
        to, bit = i, 1
        while bit <= k:
            if k & bit:
                to = to + bit * (1 - 2 * ((i // bit) % 2))
            bit *= 2
        return to

    def y_up(q):
        return lax.rem(y + q, ny)

    def remote(src, dst, s, r, who):
        return pltpu.make_async_remote_copy(
            src_ref=src, dst_ref=dst, send_sem=s, recv_sem=r, device_id=who, device_id_type=MESH
        )

    def took(ref, sem):
        remote(ref, ref, sem, sem, peer).wait_recv()

    barrier = pltpu.get_barrier_semaphore()
    for k in range(1, n_sp):
        pl.semaphore_signal(barrier, inc=1, device_id=(mate(k), t), device_id_type=MESH)
    for k in range(1, n_tp):
        pl.semaphore_signal(
            barrier, inc=1, device_id=(i, lax.rem(t + k, n_tp)), device_id_type=MESH
        )

    held = ((ids_h, ids), (wts_h, wts), (mix_h, mix), (og_h, og), (gb_h, gb), (st_h, st), (dc_h, dc))
    held = held + ((wg_h, wg), (wu_h, wu), (wd_h, wd), (wp_h, wp))
    loads = [pltpu.make_async_copy(a, b, w_sem.at[n]) for n, (a, b) in enumerate(held)]
    for load in loads:
        load.start()
    for load in loads[:4]:
        load.wait()

    with scope("build"):
        experts_iota = lax.broadcasted_iota(jnp.int32, (n_sp, tok), 0)
        named = jnp.zeros((n_sp, tok), F32)
        weight = jnp.zeros((n_sp, tok), F32)
        for k in range(ids.shape[0]):
            hit = ids[k : k + 1, :] == experts_iota
            named = jnp.where(hit, 1.0, named)
            weight = jnp.where(hit, wts[k : k + 1, :], weight)
        earlier = (
            lax.broadcasted_iota(jnp.int32, (tok, tok), 0)
            < lax.broadcasted_iota(jnp.int32, (tok, tok), 1)
        )
        place = dot(named.astype(BF16), jnp.where(earlier, 1.0, 0.0).astype(BF16), 1, 0)
        place = jnp.where(named > 0.5, place, -1.0).astype(jnp.int32)
        slot_iota = lax.broadcasted_iota(jnp.int32, (cap, tok), 0)
        for e in range(n_sp):
            here = jnp.where(place[e : e + 1, :] == slot_iota, 1.0, 0.0)
            slot_weight = jnp.sum(here * weight[e : e + 1, :], axis=1, keepdims=True)
            sel[e * cap : (e + 1) * cap, :] = here.astype(BF16)
            sw[e * cap : (e + 1) * cap, :] = jnp.broadcast_to(slot_weight, (cap, sw.shape[1]))
        chosen = sel[...]
        cols = columns(t)
        send[0, 0] = dot(chosen, mix[:, cols], 1, 0).astype(BF16).reshape(n_sp, cap, dg)
        send[1, 0] = (
            (dot(chosen, og[:, cols], 1, 0) * sw[:, 0:1]).astype(BF16).reshape(n_sp, cap, dg)
        )
        for k in straight:
            to = mate(k)
            at = pl.ds(pl.multiple_of(to * cap, cap), cap)
            for q in range(1, ny):
                cols = columns(2 * y_up(q) + c)
                send[0, q, to] = dot(sel[at, :], mix[:, cols], 1, 0).astype(BF16)
                send[1, q, to] = (dot(sel[at, :], og[:, cols], 1, 0) * sw[at, 0:1]).astype(BF16)
    with scope("barrier"):
        pl.semaphore_wait(barrier, n_sp + n_tp - 2)

    def groups(k):
        return range(ny) if k in straight else range(1)

    def dispatch(q, k):
        return remote(
            send.at[:, q, mate(k)],
            xc.at[:, 2 * y_up(q) + c, i],
            put.at[0 if q == 0 else 1],
            sp_r.at[k if q == 0 else n_sp + straight.index(k) * (ny - 1) + q - 1],
            (mate(k), t),
        )

    for k in range(1, n_sp):
        for q in groups(k):
            dispatch(q, k).start()

    with scope("own"):
        mine = pl.ds(pl.multiple_of(i * cap, cap), cap)
        here, slot_weight = sel[mine, :], sw[mine, 0:1]
        for g in range(n_tp):
            cols = slice(g * dg, (g + 1) * dg)
            xc[0, g, i] = dot(here, mix[:, cols], 1, 0).astype(BF16)
            xc[1, g, i] = (dot(here, og[:, cols], 1, 0) * slot_weight).astype(BF16)
        for load in loads[4:7]:
            load.wait()
        ga[i] = (gb[...].astype(F32) * st[...]).astype(BF16)
    pv_copy = remote(
        st.at[pl.ds(tok - 8, 8)], pv, put.at[2], one_r.at[0], (lax.rem(i + 1, n_sp), t)
    )
    pv_copy.start()

    def chunk_of(k):
        return [first <= k < end for first, end in bounds].index(True)

    def to_core(q, k):
        block = xc.at[:, 2 * y_up(q) + c, mate(k)]
        return remote(block, block, put.at[3], core_r.at[chunk_of(k)], peer)

    def to_y(q, k):
        block = xc.at[:, t, mate(k)]
        return remote(block, block, put.at[4], y_r.at[q - 1, k], (i, 2 * y_up(q) + c))

    def from_y(q, k):
        block = xc.at[:, 2 * y_up(ny - q) + c, mate(k)]
        took(block, y_r.at[q - 1, k])

    def from_sp(q, k):
        took(xc.at[:, 2 * y_up(q) + c, mate(k)], sp_r.at[k if q == 0 else n_sp + straight.index(k) * (ny - 1) + q - 1])

    def chunk(m):
        return [k for k in range(*bounds[m]) if k]

    def piece(p):
        return range(p * quarter, (p + 1) * quarter)

    def rows_of(p):
        return pl.ds(p * quarter * cap, quarter * cap)

    def spread(ks):
        for k in ks:
            with scope(f"spread{k}"):
                for q in groups(k):
                    from_sp(q, k)
                if k not in straight:
                    for q in range(1, ny):
                        to_y(q, k).start()
                for q in groups(k):
                    to_core(q, k).start()

    def hand_on(ks):
        for k in ks:
            if k in straight:
                continue
            with scope(f"hand{k}"):
                for q in range(1, ny):
                    from_y(q, k)
                    to_core(ny - q, k).start()

    def arrived(m):
        with scope(f"arr{m}"):
            took(xc.at[:, :ny, : len(chunk(m))], core_r.at[m])

    def expert(m):
        order = [mate(k) for k in range(*bounds[m])]

        def gathered(which, g):
            return jnp.concatenate([xc[which, g, s] for s in order], axis=0)

        gate = up = hg = None
        for g in range(n_tp):
            cols = slice(g * dg, (g + 1) * dg)
            x, cot = gathered(0, g), gathered(1, g)
            parts = (dot(x, wg[:, cols], 1, 1), dot(x, wu[:, cols], 1, 1), dot(cot, wd[:, cols], 1, 1))
            if g == 0:
                gate, up, hg = parts
            else:
                gate, up, hg = gate + parts[0], up + parts[1], hg + parts[2]
        s = jax.nn.sigmoid(gate)
        silu = gate * s
        hidden = (silu * up).astype(BF16)
        up_grad = (hg * silu).astype(BF16)
        gate_grad = (hg * up * s * (1.0 + gate * (1.0 - s))).astype(BF16)
        for q, src in enumerate(order):
            part = slice(q * cap, (q + 1) * cap)
            hid[src] = hidden[part]
            ug[src] = up_grad[part]
            gg[src] = gate_grad[part]
        return gate_grad, up_grad

    def partial(gate_grad, up_grad, g):
        cols = columns(g)
        return (dot(gate_grad, wg[:, cols], 1, 0) + dot(up_grad, wu[:, cols], 1, 0)).astype(BF16)

    def swap_core(p, q):
        rows = rows_of(p)
        return remote(pb.at[q, rows], rc.at[q, rows], put.at[5], pc_r.at[p, q], peer)

    def swap_y(p, q):
        rows = rows_of(p)
        return remote(
            qb.at[q, rows], ry.at[q, rows], put.at[6], py_r.at[p, q - 1], (i, 2 * y_up(q) + c)
        )

    def run(m):
        arrived(m)
        with scope(f"exp{m}"):
            grads = expert(m)
        rows = pl.ds(bounds[m][0] * cap, (bounds[m][1] - bounds[m][0]) * cap)
        with scope(f"part{m}"):
            for q in list(range(1, ny)) + [0]:
                pb[q, rows] = partial(*grads, 2 * y_up(q) + 1 - c)
                for p in reversed(pieces[m]):
                    swap_core(p, q).start()
            for q in list(range(1, ny)) + [0]:
                po[q, rows] = partial(*grads, 2 * y_up(q) + c)

    def fold_core(p):
        rows = rows_of(p)
        with scope(f"foldc{p}"):
            for q in range(1, ny):
                took(rc.at[q, rows], pc_r.at[p, q])
                qb[q, rows] = (po[q, rows].astype(F32) + rc[q, rows].astype(F32)).astype(BF16)
                swap_y(p, q).start()

    def home(k):
        return remote(
            fb.at[pl.ds(k * cap, cap)], ret.at[i], put.at[7], one_r.at[1], (mate(k), t)
        )

    def fold_y(p):
        rows = rows_of(p)
        with scope(f"foldy{p}"):
            took(rc.at[0, rows], pc_r.at[p, 0])
            total = po[0, rows].astype(F32) + rc[0, rows].astype(F32)
            for q in range(1, ny):
                took(ry.at[q, rows], py_r.at[p, q - 1])
                total = total + ry[q, rows].astype(F32)
            total = total.astype(BF16)
            fb[rows] = total
            if p == 0:
                ret[i] = total[:cap]
            for k in piece(p):
                if k:
                    home(k).start()

    def weight_grad(left, which, out):
        with scope("wgrad"):
            a = left[...].reshape(slots, left.shape[2])
            for g in range(n_tp):
                b = xc[which, g].reshape(slots, dg)
                out[:, g * dg : (g + 1) * dg] = dot(a, b, 0, 0).astype(BF16)

    level = i // quarter

    def gated_block(d):
        return ga.at[i + d * quarter]

    def send_gated(d, way):
        block = gated_block(-d * way)
        remote(block, block, put.at[8], ga_r.at[d, (1 - way) // 2], (i + way * quarter, t)).start()

    def share_gated():
        pl.when(level < 3)(lambda: send_gated(0, 1))
        pl.when(level > 0)(lambda: send_gated(0, -1))

    def relay_gated(d):
        with scope(f"relay{d}"):

            @pl.when(level >= d)
            def _():
                took(gated_block(-d), ga_r.at[d - 1, 0])
                pl.when(level < 3)(lambda: send_gated(d, 1))

            @pl.when(level + d < 4)
            def _():
                took(gated_block(d), ga_r.at[d - 1, 1])
                pl.when(level > 0)(lambda: send_gated(d, -1))

    def pass_gated(k):
        for n in range(4):
            block = ga.at[n * quarter + i % quarter]
            remote(block, block, put.at[12], one_r.at[3], (mate(k), t)).start()

    near = chunk(0)
    spread(near[1:])
    spread(near[:1])
    spread(chunk(1))
    hand_on(chunk(0))
    for load in loads[7:]:
        load.wait()
    run(0)
    spread(chunk(2))
    fold_core(1)
    share_gated()
    hand_on(chunk(1))
    run(1)
    fold_core(2)
    fold_core(0)
    hand_on(chunk(2))
    relay_gated(1)
    run(2)
    fold_core(3)
    relay_gated(2)
    fold_y(1)
    fold_y(2)
    fold_y(0)
    weight_grad(gg, 0, dwg)
    fold_y(3)
    weight_grad(ug, 0, dwu)
    weight_grad(hid, 1, dwd)
    with scope("gated"):
        relay_gated(3)
        for k in range(1, quarter):
            pass_gated(k)

    with scope("ret"):
        took(ret.at[pl.ds(1, n_sp - 1)], one_r.at[1])
    with scope("mid"):
        routed = dot(ret[...].reshape(slots, dg), sel[...], 0, 0)
        mid = (og[:, columns(t)].astype(F32).T + routed).astype(BF16)
        mt[t] = mid

    def mid_core(q):
        block = mt.at[2 * y_up(q) + c]
        return remote(block, block, put.at[9], one_r.at[4], peer)

    def mid_y(q):
        return remote(mt.at[t], mt.at[t], put.at[9], mty_r.at[q - 1], (i, 2 * y_up(q) + c))

    for q in range(1, ny):
        mid_y(q).start()
    mid_core(0).start()

    part = mr.shape[2]
    share = 2 * part
    per = dg // share
    others = [(1, n_sp // 2), (n_sp // 2, 3 * n_sp // 4), (3 * n_sp // 4, n_sp)]

    def share_rows(k):
        s = mate(k)
        first = pl.multiple_of((s % per) * share + c * part, part)
        group = [first <= k < end for first, end in others].index(True)
        return remote(
            mt.at[s // per, pl.ds(first, part)], mr.at[k, c], put.at[10], mr_r.at[group], (s, t)
        )

    def pass_rows(n):
        with scope(f"rows{n}"):
            first, end = others[n]
            block = mr.at[pl.ds(first, end - first), c]
            took(block, mr_r.at[n])
            remote(block, block, put.at[11], one_r.at[6], peer).start()

    width = dc.shape[1]
    row = lax.broadcasted_iota(jnp.int32, dc.shape, 0)
    decay = dc[...]
    head = decay[0:1, :]
    factor = jnp.where(row < tok - 1, pltpu.roll(decay, tok - 1, 0), 1.0)
    with scope("midx"):
        for q in range(1, ny):
            took(mt.at[2 * y_up(ny - q) + c], mty_r.at[q - 1])
            mid_core(ny - q).start()

    with scope("midc"):
        took(mt.at[pl.ds(0, ny)], one_r.at[4])
    for k in range(n_sp - 1, 0, -1):
        share_rows(k).start()

    with scope("scan"):
        act = dot(mt[...].reshape(n_tp * dg, tok), wp[...], 0, 0)
        grad = act * gb[...].astype(F32)
        gbr[...] = (act * st[...]).astype(BF16)
        step = 1
        while step < tok:
            inside = row < tok - step
            grad = grad + jnp.where(inside, factor * pltpu.roll(grad, tok - step, 0), 0.0)
            factor = factor * jnp.where(inside, pltpu.roll(factor, tok - step, 0), 1.0)
            step *= 2
        cs[...] = jnp.zeros(cs.shape, F32)
        for j in range(width // 128):
            lanes = slice(j * 128, (j + 1) * 128)
            cs[j : j + 1, :] = head[:, lanes] * factor[0:1, lanes]
            cs[width // 128 + j : width // 128 + j + 1, :] = head[:, lanes] * grad[0:1, lanes]

    def share_carry(k):
        return remote(cs, cr.at[i], put.at[13], one_r.at[5], (mate(k), t))

    for k in range(n_sp - 1, 0, -1):
        share_carry(k).start()

    for n in range(3):
        pass_rows(n)
    with scope("passed"):
        took(ga.at[pl.ds(0, 4 * (quarter - 1))], one_r.at[3])
    with scope("gproj0"):
        own = mt[i // per, pl.ds(pl.multiple_of((i % per) * share, share), share)]
        total = dot(own, ga[i], 1, 0)
    with scope("rowsc"):
        took(mr.at[pl.ds(1, n_sp - 1), 0], one_r.at[6])
    with scope("gproj"):
        for k in range(1, n_sp):
            total = total + dot(mr[k].reshape(share, tok), ga[mate(k)], 1, 0)
        gproj[...] = total

    with scope("carry"):
        took(cr.at[pl.ds(1, n_sp - 1)], one_r.at[5])

        def lane_row(s, first):
            return jnp.concatenate(
                [cr[s, first + j : first + j + 1, :] for j in range(width // 128)], axis=1
            )

        carry = jnp.zeros((1, width), F32)
        for s in range(n_sp - 1, 0, -1):
            carry = jnp.where(s > i, lane_row(s, width // 128) + lane_row(s, 0) * carry, carry)
        drive = grad + factor * carry
        gdr[...] = drive
        pv_copy.wait_recv()
        states = st[...]
        last = jnp.where(i > 0, pv[7:8, :], 0.0)
        previous = jnp.where(row == 0, last, pltpu.roll(states, 1, 0))
        gdc[...] = drive * previous

    with scope("drain"):
        took(xc.at[:, 0, pl.ds(1, n_sp - 1)], put.at[0])
        took(xc.at[:, pl.ds(0, ny - 1), pl.ds(0, len(straight))], put.at[1])
        pv_copy.wait_send()
        took(xc.at[:, pl.ds(0, ny), pl.ds(1, n_sp - 1)], put.at[3])
        took(xc.at[:, pl.ds(0, ny - 1), pl.ds(0, n_sp - 1 - len(straight))], put.at[4])
        took(pb, put.at[5])
        took(qb.at[pl.ds(1, ny - 1)], put.at[6])
        took(fb.at[pl.ds(cap, (n_sp - 1) * cap)], put.at[7])
        middle = level * (3 - level) > 0
        pl.when(middle)(lambda: took(ga.at[pl.ds(0, 5)], put.at[8]))
        pl.when(jnp.logical_not(middle))(lambda: took(ga.at[0], put.at[8]))
        took(ga.at[pl.ds(0, 4 * (quarter - 1))], put.at[12])
        took(mt.at[pl.ds(1, n_tp - 1)], put.at[9])
        took(mr.at[pl.ds(1, n_sp - 1), 0], put.at[10])
        took(mr.at[pl.ds(1, n_sp - 1), 0], put.at[11])
        took(cr.at[pl.ds(1, n_sp - 1)], put.at[13])


def settle(count, *refs):
    ins, outs, sem = refs[:count], refs[count : 2 * count], refs[2 * count]
    puts = [pltpu.make_async_copy(ins[n], outs[n], sem.at[n]) for n in range(count)]
    for put in puts:
        put.start()
    for put in puts:
        put.wait()


def local(
    mixer_out,
    out_grad,
    route_ids,
    route_weights,
    gate_branch,
    states,
    decay,
    w_proj,
    w_gate,
    w_up,
    w_down,
):
    tok, width = mixer_out.shape
    top = route_ids.shape[1]
    n_sp, n_tp = lax.axis_size("sp"), lax.axis_size("tp")
    ny = n_tp // 2
    assert w_gate.shape[0] == 1
    cap = 2 * top * tok // n_sp
    dg = width // n_tp
    hidden = w_gate.shape[1]
    channels = states.shape[1]
    share = width // n_sp
    vmem = pl.BlockSpec(memory_space=pltpu.VMEM)
    hbm = pl.BlockSpec(memory_space=pltpu.HBM)
    dma = pltpu.SemaphoreType.DMA
    weight = (hidden, width)
    outs = pl.pallas_call(
        functools.partial(kernel, n_sp, n_tp),
        out_shape=[jax.ShapeDtypeStruct(weight, BF16)] * 3
        + [
            jax.ShapeDtypeStruct((share, channels), F32),
            jax.ShapeDtypeStruct((tok, channels), BF16),
            jax.ShapeDtypeStruct((tok, channels), F32),
            jax.ShapeDtypeStruct((tok, channels), F32),
        ],
        in_specs=[hbm] * 11,
        out_specs=[vmem] * 7,
        scratch_shapes=[
            pltpu.VMEM((top, tok), jnp.int32),
            pltpu.VMEM((top, tok), F32),
            pltpu.VMEM((tok, width), BF16),
            pltpu.VMEM((tok, width), BF16),
            pltpu.VMEM((tok, channels), BF16),
            pltpu.VMEM((tok, channels), F32),
            pltpu.VMEM((tok, channels), F32),
            pltpu.VMEM((width, channels), BF16),
            *([pltpu.VMEM(weight, BF16)] * 3),
            pltpu.VMEM((n_sp * cap, tok), BF16),
            pltpu.VMEM((n_sp * cap, 128), F32),
            pltpu.VMEM((2, ny, n_sp, cap, dg), BF16),
            pltpu.VMEM((2, n_tp, n_sp, cap, dg), BF16),
            pltpu.VMEM((n_sp, tok, channels), BF16),
            pltpu.VMEM((8, channels), F32),
            *([pltpu.VMEM((n_sp, cap, hidden), BF16)] * 3),
            *([pltpu.VMEM((ny, n_sp * cap, dg), BF16)] * 5),
            pltpu.VMEM((n_sp * cap, dg), BF16),
            pltpu.VMEM((n_sp, cap, dg), BF16),
            pltpu.VMEM((n_tp, dg, tok), BF16),
            pltpu.VMEM((n_sp, 2, share // 2, tok), BF16),
            pltpu.VMEM((max(8, channels // 64), 128), F32),
            pltpu.VMEM((n_sp, max(8, channels // 64), 128), F32),
            dma((11,)),
            dma((14,)),
            dma((7,)),
            dma((n_sp + len(STRAIGHT) * (ny - 1),)),
            dma((3,)),
            dma((ny - 1, n_sp)),
            dma((4, ny)),
            dma((4, ny - 1)),
            dma((ny - 1,)),
            dma((3,)),
            dma((4, 2)),
        ],
        compiler_params=pltpu.CompilerParams(
            collective_id=0, has_side_effects=True, vmem_limit_bytes=LIMIT
        ),
    )(
        *(
            pltpu.with_memory_space_constraint(x, pltpu.HBM)
            for x in (
                route_ids.T,
                route_weights.T,
                mixer_out,
                out_grad,
                gate_branch,
                states,
                decay,
                w_proj,
                w_gate[0],
                w_up[0],
                w_down[0],
            )
        )
    )
    count = len(outs)
    outs = pl.pallas_call(
        functools.partial(settle, count),
        out_shape=[jax.ShapeDtypeStruct(o.shape, o.dtype) for o in outs],
        in_specs=[vmem] * count,
        out_specs=[hbm] * count,
        scratch_shapes=[dma((count,))],
        compiler_params=pltpu.CompilerParams(vmem_limit_bytes=LIMIT),
    )(*outs)
    return (outs[0][None], outs[1][None], outs[2][None], *outs[3:])


def solution(mesh):
    placed = (
        P("sp", None),
        P("sp", None),
        P("sp", None),
        P("sp", None),
        P("sp", "tp"),
        P("sp", "tp"),
        P("sp", "tp"),
        P(None, "tp"),
        P("sp", "tp", None),
        P("sp", "tp", None),
        P("sp", "tp", None),
    )
    return jax.shard_map(
        local,
        mesh=mesh,
        in_specs=placed,
        out_specs=(
            P("sp", "tp", None),
            P("sp", "tp", None),
            P("sp", "tp", None),
            P("sp", "tp"),
            P("sp", "tp"),
            P("sp", "tp"),
            P("sp", "tp"),
        ),
        check_vma=False,
    )
```

```python
import functools

import jax
import jax.numpy as jnp
from jax import lax
from jax.experimental import pallas as pl
from jax.experimental.pallas import tpu as pltpu
from jax.sharding import PartitionSpec as P

MESH = pl.DeviceIdType.MESH
F32 = jnp.float32
BF16 = jnp.bfloat16
STRAIGHT = (1, 3)
LIMIT = 44 * 1024 * 1024


def dot(a, b, ca, cb):
    return lax.dot_general(a, b, (((ca,), (cb,)), ((), ())), preferred_element_type=F32)


def kernel(
    n_sp,
    n_tp,
    ids_h,
    wts_h,
    mix_h,
    og_h,
    gb_h,
    st_h,
    dc_h,
    wp_h,
    wg_h,
    wu_h,
    wd_h,
    dwg,
    dwu,
    dwd,
    gproj,
    gbr,
    gdr,
    gdc,
    ids,
    wts,
    mix,
    og,
    gb,
    st,
    dc,
    wp,
    wg,
    wu,
    wd,
    sel,
    sw,
    send,
    xc,
    ga,
    pv,
    gg,
    ug,
    hid,
    pb,
    po,
    rc,
    qb,
    ry,
    fb,
    ret,
    mt,
    mr,
    cs,
    cr,
    w_sem,
    put,
    one_r,
    sp_r,
    core_r,
    y_r,
    pc_r,
    py_r,
    mty_r,
    mr_r,
    ga_r,
):
    i = lax.axis_index("sp")
    t = lax.axis_index("tp")
    ny = n_tp // 2
    y, c = t // 2, t % 2
    tok = mix.shape[0]
    cap = xc.shape[3]
    dg = xc.shape[4]
    slots = n_sp * cap
    peer = (i, y * 2 + 1 - c)
    straight = STRAIGHT
    quarter = n_sp // 4
    bounds = ((0, n_sp // 2), (n_sp // 2, 3 * n_sp // 4), (3 * n_sp // 4, n_sp))
    pieces = ((0, 1), (2,), (3,))
    scope = jax.named_scope

    def columns(g):
        return pl.ds(pl.multiple_of(g * dg, dg), dg)

    def mate(k):
        to, bit = i, 1
        while bit <= k:
            if k & bit:
                to = to + bit * (1 - 2 * ((i // bit) % 2))
            bit *= 2
        return to

    def y_up(q):
        return lax.rem(y + q, ny)

    def remote(src, dst, s, r, who):
        return pltpu.make_async_remote_copy(
            src_ref=src, dst_ref=dst, send_sem=s, recv_sem=r, device_id=who, device_id_type=MESH
        )

    def took(ref, sem):
        remote(ref, ref, sem, sem, peer).wait_recv()

    barrier = pltpu.get_barrier_semaphore()
    for k in range(1, n_sp):
        pl.semaphore_signal(barrier, inc=1, device_id=(mate(k), t), device_id_type=MESH)
    for k in range(1, n_tp):
        pl.semaphore_signal(
            barrier, inc=1, device_id=(i, lax.rem(t + k, n_tp)), device_id_type=MESH
        )

    held = ((ids_h, ids), (wts_h, wts), (mix_h, mix), (og_h, og), (gb_h, gb), (st_h, st), (dc_h, dc))
    held = held + ((wg_h, wg), (wu_h, wu), (wd_h, wd), (wp_h, wp))
    loads = [pltpu.make_async_copy(a, b, w_sem.at[n]) for n, (a, b) in enumerate(held)]
    for load in loads:
        load.start()
    for load in loads[:4]:
        load.wait()

    with scope("build"):
        experts_iota = lax.broadcasted_iota(jnp.int32, (n_sp, tok), 0)
        named = jnp.zeros((n_sp, tok), F32)
        weight = jnp.zeros((n_sp, tok), F32)
        for k in range(ids.shape[0]):
            hit = ids[k : k + 1, :] == experts_iota
            named = jnp.where(hit, 1.0, named)
            weight = jnp.where(hit, wts[k : k + 1, :], weight)
        earlier = (
            lax.broadcasted_iota(jnp.int32, (tok, tok), 0)
            < lax.broadcasted_iota(jnp.int32, (tok, tok), 1)
        )
        place = dot(named.astype(BF16), jnp.where(earlier, 1.0, 0.0).astype(BF16), 1, 0)
        place = jnp.where(named > 0.5, place, -1.0).astype(jnp.int32)
        slot_iota = lax.broadcasted_iota(jnp.int32, (cap, tok), 0)
        for e in range(n_sp):
            here = jnp.where(place[e : e + 1, :] == slot_iota, 1.0, 0.0)
            slot_weight = jnp.sum(here * weight[e : e + 1, :], axis=1, keepdims=True)
            sel[e * cap : (e + 1) * cap, :] = here.astype(BF16)
            sw[e * cap : (e + 1) * cap, :] = jnp.broadcast_to(slot_weight, (cap, sw.shape[1]))
        chosen = sel[...]
        cols = columns(t)
        send[0, 0] = dot(chosen, mix[:, cols], 1, 0).astype(BF16).reshape(n_sp, cap, dg)
        send[1, 0] = (
            (dot(chosen, og[:, cols], 1, 0) * sw[:, 0:1]).astype(BF16).reshape(n_sp, cap, dg)
        )
        for k in straight:
            to = mate(k)
            at = pl.ds(pl.multiple_of(to * cap, cap), cap)
            for q in range(1, ny):
                cols = columns(2 * y_up(q) + c)
                send[0, q, to] = dot(sel[at, :], mix[:, cols], 1, 0).astype(BF16)
                send[1, q, to] = (dot(sel[at, :], og[:, cols], 1, 0) * sw[at, 0:1]).astype(BF16)
    with scope("barrier"):
        pl.semaphore_wait(barrier, n_sp + n_tp - 2)

    def groups(k):
        return range(ny) if k in straight else range(1)

    def dispatch(q, k):
        return remote(
            send.at[:, q, mate(k)],
            xc.at[:, 2 * y_up(q) + c, i],
            put.at[0 if q == 0 else 1],
            sp_r.at[k if q == 0 else n_sp + straight.index(k) * (ny - 1) + q - 1],
            (mate(k), t),
        )

    for k in range(1, n_sp):
        for q in groups(k):
            dispatch(q, k).start()

    with scope("own"):
        mine = pl.ds(pl.multiple_of(i * cap, cap), cap)
        here, slot_weight = sel[mine, :], sw[mine, 0:1]
        for g in range(n_tp):
            cols = slice(g * dg, (g + 1) * dg)
            xc[0, g, i] = dot(here, mix[:, cols], 1, 0).astype(BF16)
            xc[1, g, i] = (dot(here, og[:, cols], 1, 0) * slot_weight).astype(BF16)
        for load in loads[4:7]:
            load.wait()
        ga[i] = (gb[...].astype(F32) * st[...]).astype(BF16)
    pv_copy = remote(
        st.at[pl.ds(tok - 8, 8)], pv, put.at[2], one_r.at[0], (lax.rem(i + 1, n_sp), t)
    )
    pv_copy.start()

    def chunk_of(k):
        return [first <= k < end for first, end in bounds].index(True)

    def to_core(q, k):
        block = xc.at[:, 2 * y_up(q) + c, mate(k)]
        return remote(block, block, put.at[3], core_r.at[chunk_of(k)], peer)

    def to_y(q, k):
        block = xc.at[:, t, mate(k)]
        return remote(block, block, put.at[4], y_r.at[q - 1, k], (i, 2 * y_up(q) + c))

    def from_y(q, k):
        block = xc.at[:, 2 * y_up(ny - q) + c, mate(k)]
        took(block, y_r.at[q - 1, k])

    def from_sp(q, k):
        took(xc.at[:, 2 * y_up(q) + c, mate(k)], sp_r.at[k if q == 0 else n_sp + straight.index(k) * (ny - 1) + q - 1])

    def chunk(m):
        return [k for k in range(*bounds[m]) if k]

    def piece(p):
        return range(p * quarter, (p + 1) * quarter)

    def rows_of(p):
        return pl.ds(p * quarter * cap, quarter * cap)

    def spread(ks):
        for k in ks:
            with scope(f"spread{k}"):
                for q in groups(k):
                    from_sp(q, k)
                if k not in straight:
                    for q in range(1, ny):
                        to_y(q, k).start()
                for q in groups(k):
                    to_core(q, k).start()

    def hand_on(ks):
        for k in ks:
            if k in straight:
                continue
            with scope(f"hand{k}"):
                for q in range(1, ny):
                    from_y(q, k)
                    to_core(ny - q, k).start()

    def arrived(m):
        with scope(f"arr{m}"):
            took(xc.at[:, :ny, : len(chunk(m))], core_r.at[m])

    def expert(m):
        order = [mate(k) for k in range(*bounds[m])]

        def gathered(which, g):
            return jnp.concatenate([xc[which, g, s] for s in order], axis=0)

        gate = up = hg = None
        for g in range(n_tp):
            cols = slice(g * dg, (g + 1) * dg)
            x, cot = gathered(0, g), gathered(1, g)
            parts = (dot(x, wg[:, cols], 1, 1), dot(x, wu[:, cols], 1, 1), dot(cot, wd[:, cols], 1, 1))
            if g == 0:
                gate, up, hg = parts
            else:
                gate, up, hg = gate + parts[0], up + parts[1], hg + parts[2]
        s = jax.nn.sigmoid(gate)
        silu = gate * s
        hidden = (silu * up).astype(BF16)
        up_grad = (hg * silu).astype(BF16)
        gate_grad = (hg * up * s * (1.0 + gate * (1.0 - s))).astype(BF16)
        for q, src in enumerate(order):
            part = slice(q * cap, (q + 1) * cap)
            hid[src] = hidden[part]
            ug[src] = up_grad[part]
            gg[src] = gate_grad[part]
        return gate_grad, up_grad

    def partial(gate_grad, up_grad, g):
        cols = columns(g)
        return (dot(gate_grad, wg[:, cols], 1, 0) + dot(up_grad, wu[:, cols], 1, 0)).astype(BF16)

    def swap_core(p, q):
        rows = rows_of(p)
        return remote(pb.at[q, rows], rc.at[q, rows], put.at[5], pc_r.at[p, q], peer)

    def swap_y(p, q):
        rows = rows_of(p)
        return remote(
            qb.at[q, rows], ry.at[q, rows], put.at[6], py_r.at[p, q - 1], (i, 2 * y_up(q) + c)
        )

    def run(m):
        arrived(m)
        with scope(f"exp{m}"):
            grads = expert(m)
        rows = pl.ds(bounds[m][0] * cap, (bounds[m][1] - bounds[m][0]) * cap)
        with scope(f"part{m}"):
            for q in list(range(1, ny)) + [0]:
                pb[q, rows] = partial(*grads, 2 * y_up(q) + 1 - c)
                for p in reversed(pieces[m]):
                    swap_core(p, q).start()
            for q in list(range(1, ny)) + [0]:
                po[q, rows] = partial(*grads, 2 * y_up(q) + c)

    def fold_core(p):
        rows = rows_of(p)
        with scope(f"foldc{p}"):
            for q in range(1, ny):
                took(rc.at[q, rows], pc_r.at[p, q])
                qb[q, rows] = (po[q, rows].astype(F32) + rc[q, rows].astype(F32)).astype(BF16)
                swap_y(p, q).start()

    def home(k):
        return remote(
            fb.at[pl.ds(k * cap, cap)], ret.at[i], put.at[7], one_r.at[1], (mate(k), t)
        )

    def fold_y(p):
        rows = rows_of(p)
        with scope(f"foldy{p}"):
            took(rc.at[0, rows], pc_r.at[p, 0])
            total = po[0, rows].astype(F32) + rc[0, rows].astype(F32)
            for q in range(1, ny):
                took(ry.at[q, rows], py_r.at[p, q - 1])
                total = total + ry[q, rows].astype(F32)
            total = total.astype(BF16)
            fb[rows] = total
            if p == 0:
                ret[i] = total[:cap]
            for k in piece(p):
                if k:
                    home(k).start()

    def weight_grad(left, which, out):
        with scope("wgrad"):
            a = left[...].reshape(slots, left.shape[2])
            for g in range(n_tp):
                b = xc[which, g].reshape(slots, dg)
                out[:, g * dg : (g + 1) * dg] = dot(a, b, 0, 0).astype(BF16)

    level = i // quarter

    def gated_block(d):
        return ga.at[i + d * quarter]

    def send_gated(d, way):
        block = gated_block(-d * way)
        remote(block, block, put.at[8], ga_r.at[d, (1 - way) // 2], (i + way * quarter, t)).start()

    def pass_gated(d):
        block = gated_block(d)
        for k in range(1, quarter):
            remote(block, block, put.at[12], one_r.at[3], (mate(k), t)).start()

    def share_gated():
        pl.when(level < 3)(lambda: send_gated(0, 1))
        pl.when(level > 0)(lambda: send_gated(0, -1))
        pass_gated(0)

    def relay_gated(d):
        with scope(f"relay{d}"):

            @pl.when(level >= d)
            def _():
                took(gated_block(-d), ga_r.at[d - 1, 0])
                pl.when(level < 3)(lambda: send_gated(d, 1))
                pass_gated(-d)

            @pl.when(level + d < 4)
            def _():
                took(gated_block(d), ga_r.at[d - 1, 1])
                pl.when(level > 0)(lambda: send_gated(d, -1))
                pass_gated(d)

    near = chunk(0)
    spread(near[1:])
    spread(near[:1])
    spread(chunk(1))
    hand_on(chunk(0))
    for load in loads[7:]:
        load.wait()
    run(0)
    spread(chunk(2))
    fold_core(1)
    share_gated()
    hand_on(chunk(1))
    run(1)
    fold_core(2)
    fold_core(0)
    hand_on(chunk(2))
    relay_gated(1)
    run(2)
    fold_core(3)
    relay_gated(2)
    fold_y(1)
    fold_y(2)
    fold_y(0)
    weight_grad(gg, 0, dwg)
    fold_y(3)
    weight_grad(ug, 0, dwu)
    weight_grad(hid, 1, dwd)
    with scope("gated"):
        relay_gated(3)

    with scope("ret"):
        took(ret.at[pl.ds(1, n_sp - 1)], one_r.at[1])
    with scope("mid"):
        routed = dot(ret[...].reshape(slots, dg), sel[...], 0, 0)
        mid = (og[:, columns(t)].astype(F32).T + routed).astype(BF16)
        mt[t] = mid

    def mid_core(q):
        block = mt.at[2 * y_up(q) + c]
        return remote(block, block, put.at[9], one_r.at[4], peer)

    def mid_y(q):
        return remote(mt.at[t], mt.at[t], put.at[9], mty_r.at[q - 1], (i, 2 * y_up(q) + c))

    for q in range(1, ny):
        mid_y(q).start()
    mid_core(0).start()

    part = mr.shape[2]
    share = 2 * part
    per = dg // share
    others = [(1, n_sp // 2), (n_sp // 2, 3 * n_sp // 4), (3 * n_sp // 4, n_sp)]

    def share_rows(k):
        s = mate(k)
        first = pl.multiple_of((s % per) * share + c * part, part)
        group = [first <= k < end for first, end in others].index(True)
        return remote(
            mt.at[s // per, pl.ds(first, part)], mr.at[k, c], put.at[10], mr_r.at[group], (s, t)
        )

    def pass_rows(n):
        with scope(f"rows{n}"):
            first, end = others[n]
            block = mr.at[pl.ds(first, end - first), c]
            took(block, mr_r.at[n])
            remote(block, block, put.at[11], one_r.at[6], peer).start()

    width = dc.shape[1]
    row = lax.broadcasted_iota(jnp.int32, dc.shape, 0)
    decay = dc[...]
    head = decay[0:1, :]
    factor = jnp.where(row < tok - 1, pltpu.roll(decay, tok - 1, 0), 1.0)
    with scope("midx"):
        for q in range(1, ny):
            took(mt.at[2 * y_up(ny - q) + c], mty_r.at[q - 1])
            mid_core(ny - q).start()

    with scope("midc"):
        took(mt.at[pl.ds(0, ny)], one_r.at[4])
    for k in range(n_sp - 1, 0, -1):
        share_rows(k).start()

    with scope("scan"):
        act = dot(mt[...].reshape(n_tp * dg, tok), wp[...], 0, 0)
        grad = act * gb[...].astype(F32)
        gbr[...] = (act * st[...]).astype(BF16)
        step = 1
        while step < tok:
            inside = row < tok - step
            grad = grad + jnp.where(inside, factor * pltpu.roll(grad, tok - step, 0), 0.0)
            factor = factor * jnp.where(inside, pltpu.roll(factor, tok - step, 0), 1.0)
            step *= 2
        cs[...] = jnp.zeros(cs.shape, F32)
        for j in range(width // 128):
            lanes = slice(j * 128, (j + 1) * 128)
            cs[j : j + 1, :] = head[:, lanes] * factor[0:1, lanes]
            cs[width // 128 + j : width // 128 + j + 1, :] = head[:, lanes] * grad[0:1, lanes]

    def share_carry(k):
        return remote(cs, cr.at[i], put.at[13], one_r.at[5], (mate(k), t))

    for k in range(n_sp - 1, 0, -1):
        share_carry(k).start()

    for n in range(3):
        pass_rows(n)
    with scope("passed"):
        took(ga.at[pl.ds(0, 4 * (quarter - 1))], one_r.at[3])
    with scope("gproj0"):
        own = mt[i // per, pl.ds(pl.multiple_of((i % per) * share, share), share)]
        total = dot(own, ga[i], 1, 0)
    with scope("rowsc"):
        took(mr.at[pl.ds(1, n_sp - 1), 0], one_r.at[6])
    with scope("gproj"):
        for k in range(1, n_sp):
            total = total + dot(mr[k].reshape(share, tok), ga[mate(k)], 1, 0)
        gproj[...] = total

    with scope("carry"):
        took(cr.at[pl.ds(1, n_sp - 1)], one_r.at[5])

        def lane_row(s, first):
            return jnp.concatenate(
                [cr[s, first + j : first + j + 1, :] for j in range(width // 128)], axis=1
            )

        carry = jnp.zeros((1, width), F32)
        for s in range(n_sp - 1, 0, -1):
            carry = jnp.where(s > i, lane_row(s, width // 128) + lane_row(s, 0) * carry, carry)
        drive = grad + factor * carry
        gdr[...] = drive
        pv_copy.wait_recv()
        states = st[...]
        last = jnp.where(i > 0, pv[7:8, :], 0.0)
        previous = jnp.where(row == 0, last, pltpu.roll(states, 1, 0))
        gdc[...] = drive * previous

    with scope("drain"):
        took(xc.at[:, 0, pl.ds(1, n_sp - 1)], put.at[0])
        took(xc.at[:, pl.ds(0, ny - 1), pl.ds(0, len(straight))], put.at[1])
        pv_copy.wait_send()
        took(xc.at[:, pl.ds(0, ny), pl.ds(1, n_sp - 1)], put.at[3])
        took(xc.at[:, pl.ds(0, ny - 1), pl.ds(0, n_sp - 1 - len(straight))], put.at[4])
        took(pb, put.at[5])
        took(qb.at[pl.ds(1, ny - 1)], put.at[6])
        took(fb.at[pl.ds(cap, (n_sp - 1) * cap)], put.at[7])
        middle = level * (3 - level) > 0
        pl.when(middle)(lambda: took(ga.at[pl.ds(0, 5)], put.at[8]))
        pl.when(jnp.logical_not(middle))(lambda: took(ga.at[0], put.at[8]))
        took(ga.at[pl.ds(0, 4 * (quarter - 1))], put.at[12])
        took(mt.at[pl.ds(1, n_tp - 1)], put.at[9])
        took(mr.at[pl.ds(1, n_sp - 1), 0], put.at[10])
        took(mr.at[pl.ds(1, n_sp - 1), 0], put.at[11])
        took(cr.at[pl.ds(1, n_sp - 1)], put.at[13])


def settle(count, *refs):
    ins, outs, sem = refs[:count], refs[count : 2 * count], refs[2 * count]
    puts = [pltpu.make_async_copy(ins[n], outs[n], sem.at[n]) for n in range(count)]
    for put in puts:
        put.start()
    for put in puts:
        put.wait()


def local(
    mixer_out,
    out_grad,
    route_ids,
    route_weights,
    gate_branch,
    states,
    decay,
    w_proj,
    w_gate,
    w_up,
    w_down,
):
    tok, width = mixer_out.shape
    top = route_ids.shape[1]
    n_sp, n_tp = lax.axis_size("sp"), lax.axis_size("tp")
    ny = n_tp // 2
    assert w_gate.shape[0] == 1
    cap = 2 * top * tok // n_sp
    dg = width // n_tp
    hidden = w_gate.shape[1]
    channels = states.shape[1]
    share = width // n_sp
    vmem = pl.BlockSpec(memory_space=pltpu.VMEM)
    hbm = pl.BlockSpec(memory_space=pltpu.HBM)
    dma = pltpu.SemaphoreType.DMA
    weight = (hidden, width)
    outs = pl.pallas_call(
        functools.partial(kernel, n_sp, n_tp),
        out_shape=[jax.ShapeDtypeStruct(weight, BF16)] * 3
        + [
            jax.ShapeDtypeStruct((share, channels), F32),
            jax.ShapeDtypeStruct((tok, channels), BF16),
            jax.ShapeDtypeStruct((tok, channels), F32),
            jax.ShapeDtypeStruct((tok, channels), F32),
        ],
        in_specs=[hbm] * 11,
        out_specs=[vmem] * 7,
        scratch_shapes=[
            pltpu.VMEM((top, tok), jnp.int32),
            pltpu.VMEM((top, tok), F32),
            pltpu.VMEM((tok, width), BF16),
            pltpu.VMEM((tok, width), BF16),
            pltpu.VMEM((tok, channels), BF16),
            pltpu.VMEM((tok, channels), F32),
            pltpu.VMEM((tok, channels), F32),
            pltpu.VMEM((width, channels), BF16),
            *([pltpu.VMEM(weight, BF16)] * 3),
            pltpu.VMEM((n_sp * cap, tok), BF16),
            pltpu.VMEM((n_sp * cap, 128), F32),
            pltpu.VMEM((2, ny, n_sp, cap, dg), BF16),
            pltpu.VMEM((2, n_tp, n_sp, cap, dg), BF16),
            pltpu.VMEM((n_sp, tok, channels), BF16),
            pltpu.VMEM((8, channels), F32),
            *([pltpu.VMEM((n_sp, cap, hidden), BF16)] * 3),
            *([pltpu.VMEM((ny, n_sp * cap, dg), BF16)] * 5),
            pltpu.VMEM((n_sp * cap, dg), BF16),
            pltpu.VMEM((n_sp, cap, dg), BF16),
            pltpu.VMEM((n_tp, dg, tok), BF16),
            pltpu.VMEM((n_sp, 2, share // 2, tok), BF16),
            pltpu.VMEM((max(8, channels // 64), 128), F32),
            pltpu.VMEM((n_sp, max(8, channels // 64), 128), F32),
            dma((11,)),
            dma((14,)),
            dma((7,)),
            dma((n_sp + len(STRAIGHT) * (ny - 1),)),
            dma((3,)),
            dma((ny - 1, n_sp)),
            dma((4, ny)),
            dma((4, ny - 1)),
            dma((ny - 1,)),
            dma((3,)),
            dma((4, 2)),
        ],
        compiler_params=pltpu.CompilerParams(
            collective_id=0, has_side_effects=True, vmem_limit_bytes=LIMIT
        ),
    )(
        *(
            pltpu.with_memory_space_constraint(x, pltpu.HBM)
            for x in (
                route_ids.T,
                route_weights.T,
                mixer_out,
                out_grad,
                gate_branch,
                states,
                decay,
                w_proj,
                w_gate[0],
                w_up[0],
                w_down[0],
            )
        )
    )
    count = len(outs)
    outs = pl.pallas_call(
        functools.partial(settle, count),
        out_shape=[jax.ShapeDtypeStruct(o.shape, o.dtype) for o in outs],
        in_specs=[vmem] * count,
        out_specs=[hbm] * count,
        scratch_shapes=[dma((count,))],
        compiler_params=pltpu.CompilerParams(vmem_limit_bytes=LIMIT),
    )(*outs)
    return (outs[0][None], outs[1][None], outs[2][None], *outs[3:])


def solution(mesh):
    placed = (
        P("sp", None),
        P("sp", None),
        P("sp", None),
        P("sp", None),
        P("sp", "tp"),
        P("sp", "tp"),
        P("sp", "tp"),
        P(None, "tp"),
        P("sp", "tp", None),
        P("sp", "tp", None),
        P("sp", "tp", None),
    )
    return jax.shard_map(
        local,
        mesh=mesh,
        in_specs=placed,
        out_specs=(
            P("sp", "tp", None),
            P("sp", "tp", None),
            P("sp", "tp", None),
            P("sp", "tp"),
            P("sp", "tp"),
            P("sp", "tp"),
            P("sp", "tp"),
        ),
        check_vma=False,
    )
```
